32 devices in a mesh: ep: 8 (over z, core), tp: 4 (over y, x).
Axes of the slice: x: 2, y: 2, z: 4, core: 2. Of those that a mesh axis runs over, the one named last changes fastest.
Arguments:
- tokens: bfloat16 [512, 2048], P('ep'), may hold values from -6 to 6
- mix_gain: float32 [2048], replicated, may hold values from 0.1 to 1.9
- w_in: bfloat16 [2048, 1024], P(None, 'tp'), may hold values from -0.125 to 0.125
- decay_re: float32 [64, 64], P('tp'), may hold values from -1 to -0.1
- freq: float32 [64, 64], P('tp'), may hold values from 0 to 100
- log_step: float32 [64], P('tp'), may hold values from -3.9 to 0
- in_re: bfloat16 [64, 16, 64], P('tp'), may hold values from -1 to 1
- in_im: bfloat16 [64, 16, 64], P('tp'), may hold values from -1 to 1
- out_re: bfloat16 [64, 16, 64], P('tp'), may hold values from -0.75 to 0.75
- out_im: bfloat16 [64, 16, 64], P('tp'), may hold values from -0.75 to 0.75
- skip: float32 [64, 16], P('tp'), may hold values from -4 to 4
- state_re: float32 [512, 64, 64], P('ep', 'tp'), may hold values from -6 to 6
- state_im: float32 [512, 64, 64], P('ep', 'tp'), may hold values from -6 to 6
- glu_weight: bfloat16 [1024, 1024], P(None, 'tp'), may hold values from -0.1875 to 0.1875
- glu_bias: float32 [1024], P('tp'), may hold values from -4 to 4
- out_weight: bfloat16 [1024, 2048], P('tp'), may hold values from -0.1875 to 0.1875
- ffn_gain: float32 [2048], replicated, may hold values from 0.1 to 1.9
- route: int32 [512, 2], P('ep'), may hold values from 0 to 7, all different within a row; in each aligned block of 64 rows (0 to 63, 64 to 127, ...) at most 24 rows name the same one
- route_weight: float32 [512, 2], P('ep'), may hold values from 0.2 to 1
- expert_gate: bfloat16 [8, 2048, 3584], P('ep', None, 'tp'), may hold values from -0.125 to 0.125
- expert_up: bfloat16 [8, 2048, 3584], P('ep', None, 'tp'), may hold values from -0.125 to 0.125
- expert_down: bfloat16 [8, 3584, 2048], P('ep', 'tp'), may hold values from -0.09375 to 0.09375
Outputs:
- mixed: bfloat16 [512, 2048], P('ep', 'tp')
- new_re: float32 [512, 64, 64], P('ep', 'tp')
- new_im: float32 [512, 64, 64], P('ep', 'tp')
The draws below stay inside these ranges and needn't reach their ends.
Inputs may be any that keep to these rules, and one draw needn't show every extreme that they name: `route`: each row names 2 different experts. Within the 64 rows of one index of ep no expert is named more than 24 times, and in every draw some expert is named exactly 24 times by the rows of some index of ep.
All inputs are finite; a program needn't handle non-finite values.
Results may differ from the reference program's by a relative error of at most 0.015.
Values may be sent and summed in bfloat16 or wider, within the bound.
A program may use at most 64 MiB of HBM per device.

```python
import math
import jax
import jax.numpy as jnp
import numpy as np
from jax import lax

D = 2048
C = 1024
H = 16
P_SIZE = 64
FFE = 3584
TOPK = 2
SEQ_GRP = 64
G = 64
EXPERTS = 8
SEQS = 512
CAP = 24
ROWS_E = 192
N_TP = 4


def levels(rng, shape, pieces, low, largest):
    def one(dim, blocks):
        heights = jax.random.uniform(jax.random.fold_in(jax.random.fold_in(rng, 6), dim), (blocks,), jnp.float32, low / len(pieces), largest / len(pieces))
        return jnp.repeat(jnp.exp(heights), shape[dim] // blocks).reshape((-1,) + (1,) * (len(shape) - dim - 1))

    level = one(*pieces[0])
    for cut in pieces[1:]:
        level = level * one(*cut)
    return level


def routed_block(key, own, number, rows, count, top, bound, lean):
    ranking = jax.random.permutation(key, count)
    crowded, usual = portions_of(count, rows * top, bound, lean, True), portions_of(count, rows * top, bound, lean, False)
    places = jnp.arange(count)

    def named(tallies, turn):
        used = int((tallies > 0).sum())
        fixed = max(1, used // 4)
        moved = fixed + (places - fixed + turn * (used - fixed)) % max(1, count - fixed)
        return jnp.zeros((count,), jnp.int32).at[ranking[jnp.where(places < fixed, places, moved)]].set(jnp.asarray(tallies, jnp.int32))

    tallies = jnp.where(number % 4 == 0, named(crowded, number // 4), named(usual, number - number // 4 - 1))
    mixed = jax.random.permutation(jax.random.fold_in(own, 3), count)
    donor, taker = mixed[0:count // 2 * 2:2], mixed[1:count // 2 * 2:2]
    margin = jnp.minimum(tallies[donor] - 1, bound - tallies[taker]) // 2
    margin = jnp.where((donor == ranking[0]) | (taker == ranking[0]) | (tallies[taker] == 0), 0, jnp.maximum(margin, 0))
    moved = jax.random.randint(jax.random.fold_in(own, 4), (count // 2,), 0, 1 << 20) % (margin + 1)
    tallies = tallies.at[donor].add(-moved).at[taker].add(moved)
    members = jnp.searchsorted(jnp.cumsum(tallies), jnp.arange(rows * top), side="right").astype(jnp.int32)
    listing = members.reshape(top, rows).T
    listing = listing[jax.random.permutation(jax.random.fold_in(own, 1), rows)]
    turn = jax.random.randint(jax.random.fold_in(own, 2), (rows, 1), 0, top)
    return jnp.take_along_axis(listing, (jnp.arange(top)[None, :] + turn) % top, axis=1)


def portions_of(amount, total, bound, slope, full):
    loads = [(1 << 20) // math.isqrt(rank ** slope) + 1 for rank in range(1, amount + 1)]
    largest = bound if full else min(bound, max(-(-total // amount), total * loads[0] // sum(loads)))
    least = 1 if total - largest >= amount - 1 else 0
    holding, spare = [largest] + [least] * (amount - 1), total - largest - least * (amount - 1)
    while spare > 0:
        candidates = [i for i in range(1, amount) if holding[i] < largest] or [i for i in range(1, amount) if holding[i] < bound]
        whole, budget = sum([loads[i] for i in candidates]), spare
        for i in candidates:
            addition = min(bound - holding[i], max(1, budget * loads[i] // whole), spare)
            holding[i] = holding[i] + addition
            spare = spare - addition
    return np.array(holding)


def bell_draw(rng, shape, spread, most, split=(), kind=jnp.bfloat16):
    level = levels(rng, shape, split, -0.22, 0.18) if split else 1.0
    entries = jax.random.normal(rng, shape, jnp.float32) * spread * level
    return jnp.minimum(jnp.maximum(entries, -most), most).astype(kind)


def setup_inputs(seed: int = 0) -> dict:
    splits = jax.random.split(jax.random.key(seed), 23)
    tokens = bell_draw(splits[0], (SEQS, D), 1.0, 6.0, ((0, 8),))
    mix_gain = jnp.clip(1.0 + 0.18 * jax.random.normal(splits[1], (D,), jnp.float32), 0.1, 1.9)
    w_in = bell_draw(splits[2], (D, C), D ** -0.5, 0.125, ((1, 4),))
    decay_re = jnp.clip(-1.0 + 0.9 * jax.random.uniform(splits[3], (G, P_SIZE), jnp.float32) ** levels(splits[3], (G, P_SIZE), ((0, 4),), -0.2, 0.2), -1.0, -0.1)
    freq = jnp.clip(100.0 * jax.random.uniform(splits[4], (G, P_SIZE), jnp.float32) ** levels(splits[4], (G, P_SIZE), ((0, 4),), -0.2, 0.2), 0.0, 100.0)
    log_step = jnp.clip(-3.9 + 3.9 * jax.random.uniform(splits[5], (G,), jnp.float32) ** levels(splits[5], (G,), ((0, 4),), -0.2, 0.2), -3.9, 0.0)
    in_re = bell_draw(splits[6], (G, H, P_SIZE), (2 * H) ** -0.5, 1.0, ((0, 4),))
    in_im = bell_draw(splits[7], (G, H, P_SIZE), (2 * H) ** -0.5, 1.0, ((0, 4),))
    out_re = bell_draw(splits[8], (G, H, P_SIZE), P_SIZE ** -0.5, 0.75, ((0, 4),))
    out_im = bell_draw(splits[9], (G, H, P_SIZE), P_SIZE ** -0.5, 0.75, ((0, 4),))
    skip = bell_draw(splits[10], (G, H), 1.0, 4.0, ((0, 4),), jnp.float32)
    state_re = bell_draw(splits[11], (SEQS, G, P_SIZE), 1.0, 6.0, ((0, 8), (1, 4)), jnp.float32)
    state_im = bell_draw(splits[12], (SEQS, G, P_SIZE), 1.0, 6.0, ((0, 8), (1, 4)), jnp.float32)
    glu_weight = bell_draw(splits[13], (C, C), C ** -0.5, 0.1875, ((1, 4),))
    glu_bias = bell_draw(splits[14], (C,), 1.0, 4.0, ((0, 4),), jnp.float32)
    out_weight = bell_draw(splits[15], (C, D), C ** -0.5, 0.1875, ((0, 4),))
    ffn_gain = jnp.clip(1.0 + 0.18 * jax.random.normal(splits[16], (D,), jnp.float32), 0.1, 1.9)
    route_keys = jax.random.split(jax.random.fold_in(splits[17], 1), SEQS // SEQ_GRP)
    route_turns = jax.random.permutation(jax.random.fold_in(splits[17], 3), SEQS // SEQ_GRP)
    route = jax.vmap(lambda own, number: routed_block(jax.random.fold_in(splits[17], 2), own, number, SEQ_GRP, EXPERTS, TOPK, CAP, 2))(route_keys, route_turns).reshape((SEQS, TOPK))
    route_weight = jnp.clip(0.2 + 0.8 * jax.random.uniform(splits[18], (SEQS, TOPK), jnp.float32) ** levels(splits[18], (SEQS, TOPK), ((0, 8),), -0.2, 0.2), 0.2, 1.0)
    expert_gate = bell_draw(splits[19], (EXPERTS, D, FFE), D ** -0.5, 0.125, ((0, 8), (2, 4)))
    expert_up = bell_draw(splits[20], (EXPERTS, D, FFE), D ** -0.5, 0.125, ((0, 8), (2, 4)))
    expert_down = bell_draw(splits[21], (EXPERTS, FFE, D), FFE ** -0.5, 0.09375, ((0, 8), (1, 4)))
    return {"tokens": tokens, "mix_gain": mix_gain, "w_in": w_in, "decay_re": decay_re, "freq": freq, "log_step": log_step, "in_re": in_re, "in_im": in_im, "out_re": out_re, "out_im": out_im, "skip": skip, "state_re": state_re, "state_im": state_im, "glu_weight": glu_weight, "glu_bias": glu_bias, "out_weight": out_weight, "ffn_gain": ffn_gain, "route": route, "route_weight": route_weight, "expert_gate": expert_gate, "expert_up": expert_up, "expert_down": expert_down}


norm_eps = 1e-06

def rms_scale(rows, gain):
    values = rows.astype(jnp.float32)
    scaled = values * lax.rsqrt(lax.optimization_barrier(jnp.mean(values * values, axis=-1, keepdims=True)) + norm_eps)
    return (scaled * gain).astype(jnp.bfloat16)

def split_sum(left, right, parts):
    width = left.shape[1] // parts
    lefts = jnp.moveaxis(left.reshape(left.shape[0], parts, width), 1, 0)
    rights = right.reshape(parts, width, right.shape[1])

    def add_block(total, pair):
        term = jnp.dot(pair[0], pair[1], preferred_element_type=jnp.float32).astype(jnp.bfloat16)
        term = lax.optimization_barrier(term)
        return (total + term.astype(jnp.float32), None)
    start = jnp.zeros((left.shape[0], right.shape[1]), jnp.float32)
    total, _ = lax.scan(add_block, start, (lefts, rights))
    return total

def state_step(inputs, state_re, state_im, decay_re, freq, log_step, in_re, in_im, out_re, out_im, skip):
    highest = lax.Precision.HIGHEST
    step = jnp.exp(log_step)[:, None]
    magnitude = jnp.exp(decay_re * step)
    turn_re = magnitude * jnp.cos(freq * step)
    turn_im = magnitude * jnp.sin(freq * step)
    denom = decay_re * decay_re + freq * freq
    coef_re = ((turn_re - 1.0) * decay_re + turn_im * freq) / denom
    coef_im = (turn_im * decay_re - (turn_re - 1.0) * freq) / denom
    values = inputs.astype(jnp.float32)
    drive_re = jnp.einsum('sgh,ghp->sgp', values, in_re.astype(jnp.float32), precision=highest)
    drive_im = jnp.einsum('sgh,ghp->sgp', values, in_im.astype(jnp.float32), precision=highest)
    push_re = coef_re * drive_re - coef_im * drive_im
    push_im = coef_re * drive_im + coef_im * drive_re
    new_re = turn_re * state_re - turn_im * state_im + push_re
    new_im = turn_re * state_im + turn_im * state_re + push_im
    read = jnp.einsum('ghp,sgp->sgh', out_re.astype(jnp.float32), new_re, precision=highest)
    read = read - jnp.einsum('ghp,sgp->sgh', out_im.astype(jnp.float32), new_im, precision=highest)
    read = read + skip * values
    return (read, new_re, new_im)

def reference(tokens, mix_gain, w_in, decay_re, freq, log_step, in_re, in_im, out_re, out_im, skip, state_re, state_im, glu_weight, glu_bias, out_weight, ffn_gain, route, route_weight, expert_gate, expert_up, expert_down):
    normed = rms_scale(tokens, mix_gain)
    drive = jnp.dot(normed, w_in, preferred_element_type=jnp.float32).astype(jnp.bfloat16)
    inputs = drive.reshape(SEQS, G, H)
    read, new_re, new_im = state_step(inputs, state_re, state_im, decay_re, freq, log_step, in_re, in_im, out_re, out_im, skip)
    mixed_in = jax.nn.gelu(read).reshape(SEQS, C).astype(jnp.bfloat16)
    gate = jnp.dot(mixed_in, glu_weight, preferred_element_type=jnp.float32) + glu_bias
    gated = (mixed_in.astype(jnp.float32) * jax.nn.sigmoid(gate)).astype(jnp.bfloat16)
    mix_total = split_sum(gated, out_weight, N_TP)
    resid = (tokens.astype(jnp.float32) + mix_total).astype(jnp.bfloat16)
    normed2 = rms_scale(resid, ffn_gain)
    flat_route = route.reshape(-1)
    flat_weight = route_weight.reshape(-1)

    def expert_pass(total, inputs_e):
        gate_w, up_w, down_w, index = inputs_e
        hits = flat_route == index
        picked = jnp.nonzero(hits, size=ROWS_E, fill_value=0)[0].astype(jnp.int32)
        valid = (jnp.arange(ROWS_E) < jnp.sum(hits.astype(jnp.int32))).astype(jnp.float32)
        token_ids = (picked // TOPK).astype(jnp.int32)
        rows = normed2[token_ids]
        gate_e = jnp.dot(rows, gate_w, preferred_element_type=jnp.float32)
        up_e = jnp.dot(rows, up_w, preferred_element_type=jnp.float32)
        hidden = (jax.nn.silu(gate_e) * up_e).astype(jnp.bfloat16)
        result = split_sum(hidden, down_w, N_TP).astype(jnp.bfloat16)
        weight = flat_weight[picked] * valid
        total = total.at[token_ids].add(weight[:, None] * result.astype(jnp.float32))
        return (total, None)
    start = resid.astype(jnp.float32)
    indices = jnp.arange(EXPERTS).astype(jnp.int32)
    total, _ = lax.scan(expert_pass, start, (expert_gate, expert_up, expert_down, indices))
    return (total.astype(jnp.bfloat16), new_re, new_im)
```

```python
import functools
import jax
import jax.numpy as jnp
from jax import lax
from jax.experimental import pallas as pl
from jax.experimental.pallas import tpu as pltpu
from jax.sharding import PartitionSpec as P

norm_eps = 1e-06
MESH = pl.DeviceIdType.MESH


def rms_scale(rows, gain):
    values = rows.astype(jnp.float32)
    scaled = values * lax.rsqrt(jnp.mean(values * values, axis=-1, keepdims=True) + norm_eps)
    return (scaled * gain).astype(jnp.bfloat16)


def drain(ref, sem):
    pltpu.make_async_copy(ref, ref, sem).wait()


def remote(src, dst, send, recv, axis, peer):
    copy = pltpu.make_async_remote_copy(
        src_ref=src,
        dst_ref=dst,
        send_sem=send,
        recv_sem=recv,
        device_id={axis: peer},
        device_id_type=MESH,
    )
    copy.start()


def paired(index, offset, count):
    result, bit = 0, 1
    while bit < count:
        result += lax.rem(lax.div(index, bit) + lax.div(offset, bit), 2) * bit
        bit *= 2
    return result


def each(low, high, body):
    if high - low <= 8:
        for i in range(low, high):
            body(i)
    else:
        pl.loop(low, high)(body)


def chunks_of(n_ep):
    half, quarter = n_ep // 2, n_ep // 4
    return ((0, half), (half, quarter), (half + quarter, n_ep - half - quarter))


SMALL = (
    "tokens",
    "mix_gain",
    "decay",
    "freq",
    "log_step",
    "in_re",
    "in_im",
    "w_in",
    "out_re",
    "out_im",
    "skip",
)
LATER = ("glu", "bias", "route", "weight", "out_w", "gain", "gate", "up", "down")


def mixer(v, wait, state_re, state_im, state_sem):
    f32 = jnp.float32
    bf16 = jnp.bfloat16
    groups, places, entries = v["in_re"].shape
    seqs = v["tokens"].shape[0]
    chan = v["w_in"].shape[1]

    for name in ("decay", "freq", "log_step"):
        wait(name)
    diagonal = lax.broadcasted_iota(jnp.int32, (groups, groups), 0)
    diagonal = diagonal == lax.broadcasted_iota(jnp.int32, (groups, groups), 1)
    log_step = jnp.sum(jnp.where(diagonal, v["log_step"][...], 0.0), axis=1, keepdims=True)
    step = jnp.exp(log_step)
    decay = v["decay"][...]
    freq = v["freq"][...]
    magnitude = jnp.exp(decay * step)
    turn_re = magnitude * jnp.cos(freq * step)
    turn_im = magnitude * jnp.sin(freq * step)
    denom = decay * decay + freq * freq
    coef_re = ((turn_re - 1.0) * decay + turn_im * freq) / denom
    coef_im = (turn_im * decay - (turn_re - 1.0) * freq) / denom

    def lane_group(shape):
        lane = lax.broadcasted_iota(jnp.int32, shape, len(shape) - 1)
        first = lax.broadcasted_iota(jnp.int32, shape, 0) * places
        return (lane >= first) & (lane < first + places)

    wait("tokens")
    wait("mix_gain")
    normed = rms_scale(v["tokens"][...], v["mix_gain"][...])
    wait("w_in")
    drive = jnp.dot(normed, v["w_in"][...], preferred_element_type=f32).astype(bf16)
    own_group = lane_group((groups, seqs, chan))
    apart = jnp.where(own_group, drive.astype(f32)[None], 0.0).astype(bf16)
    apart = apart.reshape(groups * seqs, chan)

    def driven(ref):
        weight = ref[...].astype(f32).reshape(chan, entries).astype(bf16)
        value = jnp.dot(apart, weight, preferred_element_type=f32)
        return value.reshape(groups, seqs, entries)

    for name in ("in_re", "in_im"):
        wait(name)
    drive_re, drive_im = driven(v["in_re"]), driven(v["in_im"])
    turn_re, turn_im = turn_re[:, None, :], turn_im[:, None, :]
    coef_re, coef_im = coef_re[:, None, :], coef_im[:, None, :]
    drain(state_re, state_sem.at[0])
    drain(state_im, state_sem.at[1])
    old_re, old_im = state_re[...], state_im[...]
    new_re = turn_re * old_re - turn_im * old_im + (coef_re * drive_re - coef_im * drive_im)
    new_im = turn_re * old_im + turn_im * old_re + (coef_re * drive_im + coef_im * drive_re)
    state_re[...] = new_re
    state_im[...] = new_im

    def read_out(value, ref):
        weight = ref[...].astype(f32).reshape(chan, entries).astype(bf16)
        value = value.reshape(groups * seqs, entries)
        high = value.astype(bf16)
        low = (value - high.astype(f32)).astype(bf16)
        dims = (((1,), (1,)), ((), ()))
        total = lax.dot_general(high, weight, dims, preferred_element_type=f32)
        return total + lax.dot_general(low, weight, dims, preferred_element_type=f32)

    for name in ("out_re", "out_im", "skip"):
        wait(name)
    spread = lax.broadcasted_iota(jnp.int32, (places, chan), 1) % places
    spread = spread == lax.broadcasted_iota(jnp.int32, (places, chan), 0)
    skip = jnp.dot(
        v["skip"][...],
        spread.astype(f32),
        precision=lax.Precision.HIGHEST,
        preferred_element_type=f32,
    )
    skip = jnp.sum(jnp.where(lane_group((groups, chan)), skip, 0.0), axis=0, keepdims=True)
    read = read_out(new_re, v["out_re"]) - read_out(new_im, v["out_im"])
    read = jnp.where(own_group, read.reshape(groups, seqs, chan), 0.0)
    read = jnp.sum(read, axis=0) + skip * drive.astype(f32)
    return jax.nn.gelu(read).astype(bf16)


def layer(n_tp, n_ep, *refs):
    f32 = jnp.float32
    bf16 = jnp.bfloat16
    names = SMALL + LATER
    hbm = dict(zip(names, refs))
    state_re_hbm, state_im_hbm, out_ref, state_re, state_im = refs[len(names) : len(names) + 5]
    rest = refs[len(names) + 5 :]
    v = dict(zip(names, rest))
    (
        mixed_ref,
        ag_buf,
        rs_out,
        rs_in,
        disp,
        rows,
        xn,
        back_out,
        back_own,
        back_in,
        ret_out,
        ret_in,
        load_sem,
        state_sem,
        ag_s,
        ag_r,
        rs_s,
        rs_r,
        disp_s,
        disp_r,
        fwd_s,
        fwd_r,
        back_s,
        back_r,
        ret_s,
        ret_r,
    ) = rest[len(names) :]
    tp = lax.axis_index("tp")
    ep = lax.axis_index("ep")
    seqs, chan = mixed_ref.shape
    width = out_ref.shape[1]
    blocks = rows.shape[2]
    slot_rows = blocks * 8
    slots = n_ep * slot_rows
    hidden_n = v["gate"].shape[1]
    peers = tuple(range(n_tp - 1, 0, -1))
    chunks = chunks_of(n_ep)

    def copy_of(name):
        src = hbm[name]
        if name in ("gate", "up", "down"):
            src = src.at[0]
        return pltpu.make_async_copy(src, v[name], load_sem.at[names.index(name)])

    def wait(name):
        copy_of(name).wait()

    for name in SMALL:
        copy_of(name).start()

    @pl.loop(0, state_re.shape[0])
    def _(g):
        for i, (far, near) in enumerate(((state_re_hbm, state_re), (state_im_hbm, state_im))):
            pltpu.make_async_copy(far.at[:, g, :], near.at[g], state_sem.at[i]).start()

    for name in LATER:
        copy_of(name).start()

    barrier = pltpu.get_barrier_semaphore()

    @pl.loop(1, n_tp)
    def _(k):
        pl.semaphore_signal(
            barrier, inc=1, device_id={"tp": lax.rem(tp + k, n_tp)}, device_id_type=MESH
        )

    @pl.loop(1, n_ep)
    def _(k):
        pl.semaphore_signal(
            barrier, inc=1, device_id={"ep": lax.rem(ep + k, n_ep)}, device_id_type=MESH
        )

    def tp_peer(k):
        return paired(tp, k, n_tp)

    def ep_peer(i):
        return paired(ep, i, n_ep)

    mixed = mixer(v, wait, state_re, state_im, state_sem)
    mixed_ref[...] = mixed
    pl.semaphore_wait(barrier, n_tp + n_ep - 2)
    for k in peers:
        remote(mixed_ref, ag_buf.at[k - 1], ag_s.at[k - 1], ag_r.at[k - 1], "tp", tp_peer(k))

    def one_hot(index, size):
        return lax.broadcasted_iota(jnp.int32, (seqs, size), 1).astype(f32) == index

    row = lax.broadcasted_iota(jnp.int32, (seqs, seqs), 0)
    lane = lax.broadcasted_iota(jnp.int32, (seqs, seqs), 1)

    def upright(ref, k):
        value = ref[k : k + 1, :].astype(f32)
        return jnp.sum(jnp.where(row == lane, value, 0.0), axis=1, keepdims=True)

    for name in ("route", "weight", "bias", "gain"):
        wait(name)
    route_ref, weight_ref, gain_ref = v["route"], v["weight"], v["gain"]
    choices = [upright(route_ref, k) for k in range(route_ref.shape[0])]
    hits = [one_hot(choice, n_ep).astype(f32) for choice in choices]
    earlier = jnp.where(lane < row, 1.0, 0.0).astype(bf16)
    before = jnp.dot(earlier, sum(hits).astype(bf16), preferred_element_type=f32)
    select = jnp.zeros((seqs, slots), f32)
    combine = jnp.zeros((seqs, slots), f32)
    for k, choice in enumerate(choices):
        rank = jnp.sum(before * hits[k], axis=1, keepdims=True)
        pick = one_hot(choice * slot_rows + rank, slots)
        select = jnp.where(pick, 1.0, select)
        combine = jnp.where(pick, upright(weight_ref, k), combine)

    def glu_rows(owner):
        return v["glu"][pl.ds(pl.multiple_of(owner * chan, chan), chan), :]

    wait("glu")
    gate = jnp.dot(mixed, glu_rows(tp), preferred_element_type=f32) + v["bias"][...]
    for k in reversed(peers):
        drain(ag_buf.at[k - 1], ag_r.at[k - 1])
        gate += jnp.dot(ag_buf[k - 1], glu_rows(tp_peer(k)), preferred_element_type=f32)
    gated = (mixed.astype(f32) * jax.nn.sigmoid(gate)).astype(bf16)

    wait("out_w")

    def columns(owner):
        return pl.ds(pl.multiple_of(owner * width, width), width)

    for k in peers:
        part = jnp.dot(gated, v["out_w"][:, columns(tp_peer(k))], preferred_element_type=f32)
        rs_out[k - 1] = part.astype(bf16)
        remote(
            rs_out.at[k - 1], rs_in.at[k - 1], rs_s.at[k - 1], rs_r.at[k - 1], "tp", tp_peer(k)
        )
    total = jnp.dot(gated, v["out_w"][:, columns(tp)], preferred_element_type=f32)
    total = total.astype(bf16).astype(f32)
    for k in reversed(peers):
        drain(rs_in.at[k - 1], rs_r.at[k - 1])
        total += rs_in[k - 1].astype(f32)
    resid = (v["tokens"][:, columns(tp)].astype(f32) + total).astype(bf16)

    picked = lax.dot_general(
        select.astype(bf16), resid, (((0,), (0,)), ((), ())), preferred_element_type=f32
    )
    disp[...] = picked.reshape(n_ep, blocks, 8, width).astype(bf16)

    def dispatch(i):
        to = ep_peer(i)
        remote(disp.at[to], rows.at[tp, i], disp_s, disp_r.at[i - 1], "ep", to)

    each(1, n_ep, dispatch)

    for k in peers:
        remote(disp.at[ep], rows.at[tp, 0], fwd_s.at[k - 1], fwd_r.at[0, k - 1], "tp", tp_peer(k))
    rows[tp, 0] = disp[ep]

    for part, (start, count) in enumerate(chunks):

        def forward(i, part=part):
            here = rows.at[tp, i]
            drain(here, disp_r.at[i - 1])
            for k in peers:
                remote(here, here, fwd_s.at[k - 1], fwd_r.at[part, k - 1], "tp", tp_peer(k))

        each(max(start, 1), start + count, forward)

    for part, (start, count) in enumerate(chunks):
        span = pl.ds(start, count)
        held = xn.at[pl.ds(0, count * slot_rows)]

        def row_values(owner):
            return rows[owner, span].astype(f32).reshape(count * slot_rows, width)

        values = row_values(tp)
        squares = jnp.sum(values * values, axis=1, keepdims=True)
        for k in reversed(peers):
            drain(rows.at[tp_peer(k), span], fwd_r.at[part, k - 1])
            values = row_values(tp_peer(k))
            squares += jnp.sum(values * values, axis=1, keepdims=True)
        scale = lax.rsqrt(squares / (n_tp * width) + norm_eps)
        for owner in range(n_tp):
            cols = pl.ds(owner * width, width)
            held[:, cols] = (row_values(owner) * scale * gain_ref[:, cols]).astype(bf16)

        if part == 0:
            wait("gate")
            wait("up")
        pieces = []
        for first in range(0, hidden_n, 256):
            cols = pl.ds(first, min(256, hidden_n - first))
            gate_h = jnp.dot(held[...], v["gate"][:, cols], preferred_element_type=f32)
            up_h = jnp.dot(held[...], v["up"][:, cols], preferred_element_type=f32)
            pieces.append((jax.nn.silu(gate_h) * up_h).astype(bf16))
        hidden = jnp.concatenate(pieces, axis=1)
        if part == 0:
            wait("down")

        def down(owner):
            value = jnp.dot(hidden, v["down"][:, columns(owner)], preferred_element_type=f32)
            return value.reshape(count, blocks, 8, width).astype(bf16)

        for k in peers:
            back_out[k - 1, span] = down(tp_peer(k))
            remote(
                back_out.at[k - 1, span],
                back_in.at[k - 1, span],
                back_s.at[k - 1],
                back_r.at[part, k - 1],
                "tp",
                tp_peer(k),
            )
        back_own[span] = down(tp)

    for part, (start, count) in enumerate(chunks):
        for k in peers:
            drain(back_in.at[k - 1, pl.ds(start, count)], back_r.at[part, k - 1])

        def settle(i):
            result = back_own[i].astype(f32)
            for k in reversed(peers):
                result += back_in[k - 1, i].astype(f32)
            result = result.astype(bf16)
            if isinstance(i, int) and i == 0:
                ret_in[ep] = result
                return
            to = ep_peer(i)
            ret_out[to] = result
            remote(ret_out.at[to], ret_in.at[ep], ret_s, ret_r.at[i - 1], "ep", to)

        if start == 0:
            settle(0)
        each(max(start, 1), start + count, settle)

    def arrived(i):
        drain(ret_in.at[ep_peer(i)], ret_r.at[i - 1])

    each(1, n_ep, arrived)

    returned = ret_in[...].astype(f32).reshape(slots, width).astype(bf16)
    high = combine.astype(bf16)
    low = (combine - high.astype(f32)).astype(bf16)
    expert_total = jnp.dot(high, returned, preferred_element_type=f32)
    expert_total += jnp.dot(low, returned, preferred_element_type=f32)
    out_ref[...] = (resid.astype(f32) + expert_total).astype(bf16)

    for k in peers:
        drain(mixed_ref, ag_s.at[k - 1])
        drain(rs_out.at[k - 1], rs_s.at[k - 1])
        drain(rows.at[0], fwd_s.at[k - 1])
        drain(back_out.at[k - 1], back_s.at[k - 1])
    drain(disp.at[pl.ds(0, n_ep - 1)], disp_s)
    drain(ret_out.at[pl.ds(0, n_ep - 1)], ret_s)


def store(mixed_ref, re_ref, im_ref, mixed_hbm, re_hbm, im_hbm, sem):
    out = pltpu.make_async_copy(mixed_ref, mixed_hbm, sem.at[0])
    out.start()

    @pl.loop(0, re_ref.shape[0])
    def _(g):
        for i, (near, far) in enumerate(((re_ref, re_hbm), (im_ref, im_hbm))):
            pltpu.make_async_copy(near.at[g], far.at[:, g, :], sem.at[i + 1]).start()

    out.wait()
    drain(re_ref, sem.at[1])
    drain(im_ref, sem.at[2])


def local(
    tokens,
    mix_gain,
    w_in,
    decay_re,
    freq,
    log_step,
    in_re,
    in_im,
    out_re,
    out_im,
    skip,
    state_re,
    state_im,
    glu_weight,
    glu_bias,
    out_weight,
    ffn_gain,
    route,
    route_weight,
    expert_gate,
    expert_up,
    expert_down,
):
    seq_count, model_width = tokens.shape
    n_tp = lax.axis_size("tp")
    experts = lax.axis_size("ep")
    local_width = model_width // n_tp
    top_count = route.shape[1]
    slot_cap = (3 * seq_count * top_count + 2 * experts - 1) // (2 * experts)
    slot_rows = (slot_cap + 7) // 8 * 8
    chan = w_in.shape[1]
    state_block = (decay_re.shape[0], seq_count, state_re.shape[2])
    block = (slot_rows // 8, 8, local_width)
    chunks = chunks_of(experts)
    bf16 = jnp.bfloat16
    dma = pltpu.SemaphoreType.DMA
    vmem = pl.BlockSpec(memory_space=pltpu.VMEM)
    anyplace = pl.BlockSpec(memory_space=pl.ANY)
    arrays = {
        "tokens": tokens,
        "mix_gain": mix_gain[None, :],
        "w_in": w_in,
        "decay": decay_re,
        "freq": freq,
        "log_step": log_step[None, :],
        "in_re": in_re,
        "in_im": in_im,
        "out_re": out_re,
        "out_im": out_im,
        "skip": skip,
        "glu": glu_weight,
        "bias": glu_bias[None, :],
        "out_w": out_weight,
        "gain": ffn_gain[None, :],
        "route": route.T,
        "weight": route_weight.T,
        "gate": expert_gate,
        "up": expert_up,
        "down": expert_down,
    }
    arrays = [arrays[name] for name in SMALL + LATER]
    holds = [
        pltpu.VMEM(a.shape[1:] if name in ("gate", "up", "down") else a.shape, a.dtype)
        for name, a in zip(SMALL + LATER, arrays)
    ]
    mixed, new_re, new_im = pl.pallas_call(
        functools.partial(layer, n_tp, experts),
        out_shape=(
            pltpu.VMEM((seq_count, local_width), bf16),
            pltpu.VMEM(state_block, jnp.float32),
            pltpu.VMEM(state_block, jnp.float32),
        ),
        in_specs=[anyplace] * (len(arrays) + 2),
        out_specs=(vmem, vmem, vmem),
        scratch_shapes=holds
        + [
            pltpu.VMEM((seq_count, chan), bf16),
            pltpu.VMEM((n_tp - 1, seq_count, chan), bf16),
            pltpu.VMEM((n_tp - 1, seq_count, local_width), bf16),
            pltpu.VMEM((n_tp - 1, seq_count, local_width), bf16),
            pltpu.VMEM((experts,) + block, bf16),
            pltpu.VMEM((n_tp, experts) + block, bf16),
            pltpu.VMEM((max(c for _, c in chunks) * slot_rows, model_width), bf16),
            pltpu.VMEM((n_tp - 1, experts) + block, bf16),
            pltpu.VMEM((experts,) + block, bf16),
            pltpu.VMEM((n_tp - 1, experts) + block, bf16),
            pltpu.VMEM((experts,) + block, bf16),
            pltpu.VMEM((experts,) + block, bf16),
            dma((len(arrays),)),
            dma((2,)),
            dma((n_tp - 1,)),
            dma((n_tp - 1,)),
            dma((n_tp - 1,)),
            dma((n_tp - 1,)),
            dma,
            dma((experts - 1,)),
            dma((n_tp - 1,)),
            dma((len(chunks), n_tp - 1)),
            dma((n_tp - 1,)),
            dma((len(chunks), n_tp - 1)),
            dma,
            dma((experts - 1,)),
        ],
        compiler_params=pltpu.CompilerParams(
            collective_id=0, has_side_effects=True, vmem_limit_bytes=58 * 1024 * 1024
        ),
    )(*arrays, state_re, state_im)
    results = [pltpu.with_memory_space_constraint(a, pltpu.VMEM) for a in (mixed, new_re, new_im)]
    return pl.pallas_call(
        store,
        out_shape=(
            jax.ShapeDtypeStruct((seq_count, local_width), bf16),
            jax.ShapeDtypeStruct(state_re.shape, jnp.float32),
            jax.ShapeDtypeStruct(state_im.shape, jnp.float32),
        ),
        in_specs=[vmem] * 3,
        out_specs=(anyplace,) * 3,
        scratch_shapes=[dma((3,))],
    )(*results)


def solution(mesh):
    in_specs = (
        P("ep", None),
        P(),
        P(None, "tp"),
        P("tp", None),
        P("tp", None),
        P("tp"),
        P("tp", None, None),
        P("tp", None, None),
        P("tp", None, None),
        P("tp", None, None),
        P("tp", None),
        P("ep", "tp", None),
        P("ep", "tp", None),
        P(None, "tp"),
        P("tp"),
        P("tp", None),
        P(),
        P("ep", None),
        P("ep", None),
        P("ep", None, "tp"),
        P("ep", None, "tp"),
        P("ep", "tp", None),
    )
    out_specs = (P("ep", "tp"), P("ep", "tp", None), P("ep", "tp", None))
    return jax.shard_map(local, mesh=mesh, in_specs=in_specs, out_specs=out_specs, check_vma=False)
```

```python
import functools
import jax
import jax.numpy as jnp
from jax import lax
from jax.experimental import pallas as pl
from jax.experimental.pallas import tpu as pltpu
from jax.sharding import PartitionSpec as P

norm_eps = 1e-06
MESH = pl.DeviceIdType.MESH


def rms_scale(rows, gain):
    values = rows.astype(jnp.float32)
    scaled = values * lax.rsqrt(jnp.mean(values * values, axis=-1, keepdims=True) + norm_eps)
    return (scaled * gain).astype(jnp.bfloat16)


def drain(ref, sem):
    pltpu.make_async_copy(ref, ref, sem).wait()


def remote(src, dst, send, recv, axis, peer):
    copy = pltpu.make_async_remote_copy(
        src_ref=src,
        dst_ref=dst,
        send_sem=send,
        recv_sem=recv,
        device_id={axis: peer},
        device_id_type=MESH,
    )
    copy.start()


def paired(index, offset, count):
    result, bit = 0, 1
    while bit < count:
        result += lax.rem(lax.div(index, bit) + lax.div(offset, bit), 2) * bit
        bit *= 2
    return result


def offset_at(place, count):
    pair, core = place // 2 * 2, place % 2
    return (count - pair) % count + core


def each(low, high, body):
    if high - low <= 8:
        for i in range(low, high):
            body(i)
    else:
        pl.loop(low, high)(body)


def chunks_of(n_ep):
    half, quarter = n_ep // 2, n_ep // 4
    return ((0, half), (half, quarter), (half + quarter, n_ep - half - quarter))


SMALL = (
    "tokens",
    "mix_gain",
    "decay",
    "freq",
    "log_step",
    "in_re",
    "in_im",
    "w_in",
    "out_re",
    "out_im",
    "skip",
)
LATER = ("glu", "bias", "route", "weight", "out_w", "gain", "gate", "up", "down")


def mixer(v, wait, state_re, state_im, state_sem):
    f32 = jnp.float32
    bf16 = jnp.bfloat16
    groups, places, entries = v["in_re"].shape
    seqs = v["tokens"].shape[0]
    chan = v["w_in"].shape[1]

    for name in ("decay", "freq", "log_step"):
        wait(name)
    diagonal = lax.broadcasted_iota(jnp.int32, (groups, groups), 0)
    diagonal = diagonal == lax.broadcasted_iota(jnp.int32, (groups, groups), 1)
    log_step = jnp.sum(jnp.where(diagonal, v["log_step"][...], 0.0), axis=1, keepdims=True)
    step = jnp.exp(log_step)
    decay = v["decay"][...]
    freq = v["freq"][...]
    magnitude = jnp.exp(decay * step)
    turn_re = magnitude * jnp.cos(freq * step)
    turn_im = magnitude * jnp.sin(freq * step)
    denom = decay * decay + freq * freq
    coef_re = ((turn_re - 1.0) * decay + turn_im * freq) / denom
    coef_im = (turn_im * decay - (turn_re - 1.0) * freq) / denom

    def lane_group(shape):
        lane = lax.broadcasted_iota(jnp.int32, shape, len(shape) - 1)
        first = lax.broadcasted_iota(jnp.int32, shape, 0) * places
        return (lane >= first) & (lane < first + places)

    wait("tokens")
    wait("mix_gain")
    normed = rms_scale(v["tokens"][...], v["mix_gain"][...])
    wait("w_in")
    drive = jnp.dot(normed, v["w_in"][...], preferred_element_type=f32).astype(bf16)
    own_group = lane_group((groups, seqs, chan))
    apart = jnp.where(own_group, drive.astype(f32)[None], 0.0).astype(bf16)
    apart = apart.reshape(groups * seqs, chan)

    def driven(ref):
        weight = ref[...].astype(f32).reshape(chan, entries).astype(bf16)
        value = jnp.dot(apart, weight, preferred_element_type=f32)
        return value.reshape(groups, seqs, entries)

    for name in ("in_re", "in_im"):
        wait(name)
    drive_re, drive_im = driven(v["in_re"]), driven(v["in_im"])
    turn_re, turn_im = turn_re[:, None, :], turn_im[:, None, :]
    coef_re, coef_im = coef_re[:, None, :], coef_im[:, None, :]
    drain(state_re, state_sem.at[0])
    drain(state_im, state_sem.at[1])
    old_re, old_im = state_re[...], state_im[...]
    new_re = turn_re * old_re - turn_im * old_im + (coef_re * drive_re - coef_im * drive_im)
    new_im = turn_re * old_im + turn_im * old_re + (coef_re * drive_im + coef_im * drive_re)
    state_re[...] = new_re
    state_im[...] = new_im

    def read_out(value, ref):
        weight = ref[...].astype(f32).reshape(chan, entries).astype(bf16)
        value = value.reshape(groups * seqs, entries)
        high = value.astype(bf16)
        low = (value - high.astype(f32)).astype(bf16)
        dims = (((1,), (1,)), ((), ()))
        total = lax.dot_general(high, weight, dims, preferred_element_type=f32)
        return total + lax.dot_general(low, weight, dims, preferred_element_type=f32)

    for name in ("out_re", "out_im", "skip"):
        wait(name)
    spread = lax.broadcasted_iota(jnp.int32, (places, chan), 1) % places
    spread = spread == lax.broadcasted_iota(jnp.int32, (places, chan), 0)
    skip = jnp.dot(
        v["skip"][...],
        spread.astype(f32),
        precision=lax.Precision.HIGHEST,
        preferred_element_type=f32,
    )
    skip = jnp.sum(jnp.where(lane_group((groups, chan)), skip, 0.0), axis=0, keepdims=True)
    read = read_out(new_re, v["out_re"]) - read_out(new_im, v["out_im"])
    read = jnp.where(own_group, read.reshape(groups, seqs, chan), 0.0)
    read = jnp.sum(read, axis=0) + skip * drive.astype(f32)
    return jax.nn.gelu(read).astype(bf16)


def gated_unit(gate, up):
    return (jax.nn.silu(gate) * up).astype(jnp.bfloat16)


def layer(n_tp, n_ep, *refs):
    f32 = jnp.float32
    bf16 = jnp.bfloat16
    names = SMALL + LATER
    hbm = dict(zip(names, refs))
    state_re_hbm, state_im_hbm, out_ref, state_re, state_im = refs[len(names) : len(names) + 5]
    rest = refs[len(names) + 5 :]
    v = dict(zip(names, rest))
    (
        mixed_ref,
        ag_buf,
        rs_out,
        rs_in,
        disp,
        rows,
        xn,
        back_out,
        back_own,
        back_in,
        ret_out,
        ret_in,
        load_sem,
        state_sem,
        ag_s,
        ag_r,
        rs_s,
        rs_r,
        disp_s,
        disp_r,
        fwd_s,
        fwd_r,
        back_s,
        back_r,
        ret_s,
        ret_r,
    ) = rest[len(names) :]
    tp = lax.axis_index("tp")
    ep = lax.axis_index("ep")
    seqs, chan = mixed_ref.shape
    width = out_ref.shape[1]
    blocks = rows.shape[2]
    slot_rows = blocks * 8
    slots = n_ep * slot_rows
    hidden_n = v["gate"].shape[1]
    peers = tuple(range(n_tp - 1, 0, -1))
    chunks = chunks_of(n_ep)
    first_part = [start for start, _ in chunks].index(0)

    def copy_of(name):
        src = hbm[name]
        if name in ("gate", "up", "down"):
            src = src.at[0]
        return pltpu.make_async_copy(src, v[name], load_sem.at[names.index(name)])

    def wait(name):
        copy_of(name).wait()

    for name in SMALL:
        copy_of(name).start()

    @pl.loop(0, state_re.shape[0])
    def _(g):
        for i, (far, near) in enumerate(((state_re_hbm, state_re), (state_im_hbm, state_im))):
            pltpu.make_async_copy(far.at[:, g, :], near.at[g], state_sem.at[i]).start()

    for name in LATER:
        copy_of(name).start()

    barrier = pltpu.get_barrier_semaphore()

    @pl.loop(1, n_tp)
    def _(k):
        pl.semaphore_signal(
            barrier, inc=1, device_id={"tp": lax.rem(tp + k, n_tp)}, device_id_type=MESH
        )

    @pl.loop(1, n_ep)
    def _(k):
        pl.semaphore_signal(
            barrier, inc=1, device_id={"ep": lax.rem(ep + k, n_ep)}, device_id_type=MESH
        )

    def tp_peer(k):
        return paired(tp, k, n_tp)

    def ep_peer(i):
        return paired(ep, offset_at(i, n_ep), n_ep)

    mixed = mixer(v, wait, state_re, state_im, state_sem)
    mixed_ref[...] = mixed
    pl.semaphore_wait(barrier, n_tp + n_ep - 2)
    for k in peers:
        remote(mixed_ref, ag_buf.at[k - 1], ag_s.at[k - 1], ag_r.at[k - 1], "tp", tp_peer(k))

    def one_hot(index, size):
        return lax.broadcasted_iota(jnp.int32, (seqs, size), 1).astype(f32) == index

    row = lax.broadcasted_iota(jnp.int32, (seqs, seqs), 0)
    lane = lax.broadcasted_iota(jnp.int32, (seqs, seqs), 1)

    def upright(ref, k):
        value = ref[k : k + 1, :].astype(f32)
        return jnp.sum(jnp.where(row == lane, value, 0.0), axis=1, keepdims=True)

    for name in ("route", "weight", "bias", "gain"):
        wait(name)
    route_ref, weight_ref, gain_ref = v["route"], v["weight"], v["gain"]
    choices = [upright(route_ref, k) for k in range(route_ref.shape[0])]
    hits = [one_hot(choice, n_ep).astype(f32) for choice in choices]
    earlier = jnp.where(lane < row, 1.0, 0.0).astype(bf16)
    before = jnp.dot(earlier, sum(hits).astype(bf16), preferred_element_type=f32)
    select = jnp.zeros((seqs, slots), f32)
    combine = jnp.zeros((seqs, slots), f32)
    for k, choice in enumerate(choices):
        rank = jnp.sum(before * hits[k], axis=1, keepdims=True)
        pick = one_hot(choice * slot_rows + rank, slots)
        select = jnp.where(pick, 1.0, select)
        combine = jnp.where(pick, upright(weight_ref, k), combine)

    def glu_rows(owner):
        return v["glu"][pl.ds(pl.multiple_of(owner * chan, chan), chan), :]

    wait("glu")
    gate = jnp.dot(mixed, glu_rows(tp), preferred_element_type=f32) + v["bias"][...]
    for k in reversed(peers):
        drain(ag_buf.at[k - 1], ag_r.at[k - 1])
        gate += jnp.dot(ag_buf[k - 1], glu_rows(tp_peer(k)), preferred_element_type=f32)
    gated = (mixed.astype(f32) * jax.nn.sigmoid(gate)).astype(bf16)

    wait("out_w")

    def columns(owner):
        return pl.ds(pl.multiple_of(owner * width, width), width)

    def share(owner):
        value = jnp.dot(gated, v["out_w"][:, columns(owner)], preferred_element_type=f32)
        return value.astype(bf16)

    shares = [share(tp_peer(k)) for k in peers] if n_tp <= 4 else None
    for at, k in enumerate(peers):
        rs_out[k - 1] = shares[at] if shares else share(tp_peer(k))
        remote(
            rs_out.at[k - 1], rs_in.at[k - 1], rs_s.at[k - 1], rs_r.at[k - 1], "tp", tp_peer(k)
        )
    total = share(tp).astype(f32)
    for k in reversed(peers):
        drain(rs_in.at[k - 1], rs_r.at[k - 1])
        total += rs_in[k - 1].astype(f32)
    resid = (v["tokens"][:, columns(tp)].astype(f32) + total).astype(bf16)

    picked = lax.dot_general(
        select.astype(bf16), resid, (((0,), (0,)), ((), ())), preferred_element_type=f32
    )
    disp[...] = picked.reshape(n_ep, blocks, 8, width).astype(bf16)

    def dispatch(i):
        to = ep_peer(i)
        remote(disp.at[to], rows.at[tp, i], disp_s, disp_r.at[i - 1], "ep", to)

    each(1, n_ep, dispatch)

    for k in peers:
        remote(disp.at[ep], rows.at[tp, 0], fwd_s.at[k - 1], fwd_r.at[first_part, k - 1], "tp", tp_peer(k))
    rows[tp, 0] = disp[ep]

    for start, part, count in sorted((start, part, count) for part, (start, count) in enumerate(chunks)):

        def forward(i, part=part):
            here = rows.at[tp, i]
            drain(here, disp_r.at[i - 1])
            for k in peers:
                remote(here, here, fwd_s.at[k - 1], fwd_r.at[part, k - 1], "tp", tp_peer(k))

        each(max(start, 1), start + count, forward)

    for part, (start, count) in enumerate(chunks):
        span = pl.ds(start, count)
        held = xn.at[pl.ds(0, count * slot_rows)]

        def row_values(owner):
            return rows[owner, span].astype(f32).reshape(count * slot_rows, width)

        for k in reversed(peers):
            drain(rows.at[tp_peer(k), span], fwd_r.at[part, k - 1])
        squares = sum(row_values(owner) * row_values(owner) for owner in range(n_tp))
        squares = jnp.sum(squares, axis=1, keepdims=True)
        scale = lax.rsqrt(squares / (n_tp * width) + norm_eps)
        for owner in range(n_tp):
            cols = pl.ds(owner * width, width)
            held[:, cols] = (row_values(owner) * scale * gain_ref[:, cols]).astype(bf16)

        if part == 0:
            wait("gate")
            wait("up")
        products = (
            jnp.dot(held[...], v[name][...], preferred_element_type=f32) for name in ("gate", "up")
        )
        hidden = gated_unit(*products)
        if part == 0:
            wait("down")

        def down(owner):
            value = jnp.dot(hidden, v["down"][:, columns(owner)], preferred_element_type=f32)
            return value.reshape(count, blocks, 8, width).astype(bf16)

        def give_back(k, value):
            back_out[k - 1, span] = value
            remote(
                back_out.at[k - 1, span],
                back_in.at[k - 1, span],
                back_s.at[k - 1],
                back_r.at[part, k - 1],
                "tp",
                tp_peer(k),
            )

        ready = None
        for k in peers:
            value = down(tp_peer(k))
            if ready is not None:
                give_back(*ready)
            ready = k, value
        own = down(tp)
        give_back(*ready)
        back_own[span] = own

    for part, (start, count) in enumerate(chunks):
        for k in peers:
            drain(back_in.at[k - 1, pl.ds(start, count)], back_r.at[part, k - 1])

        def settle(i):
            result = back_own[i].astype(f32)
            for k in reversed(peers):
                result += back_in[k - 1, i].astype(f32)
            result = result.astype(bf16)
            if isinstance(i, int) and i == 0:
                ret_in[ep] = result
                return
            to = ep_peer(i)
            ret_out[to] = result
            remote(ret_out.at[to], ret_in.at[ep], ret_s, ret_r.at[i - 1], "ep", to)

        if start == 0:
            settle(0)
        each(max(start, 1), start + count, settle)

    def arrived(i):
        drain(ret_in.at[ep_peer(i)], ret_r.at[i - 1])

    each(1, n_ep, arrived)

    returned = ret_in[...].astype(f32).reshape(slots, width).astype(bf16)
    high = combine.astype(bf16)
    low = (combine - high.astype(f32)).astype(bf16)
    expert_total = jnp.dot(high, returned, preferred_element_type=f32)
    expert_total += jnp.dot(low, returned, preferred_element_type=f32)
    out_ref[...] = (resid.astype(f32) + expert_total).astype(bf16)

    for k in peers:
        drain(mixed_ref, ag_s.at[k - 1])
        drain(rs_out.at[k - 1], rs_s.at[k - 1])
        drain(rows.at[0], fwd_s.at[k - 1])
        drain(back_out.at[k - 1], back_s.at[k - 1])
    drain(disp.at[pl.ds(0, n_ep - 1)], disp_s)
    drain(ret_out.at[pl.ds(0, n_ep - 1)], ret_s)


def store(mixed_ref, re_ref, im_ref, mixed_hbm, re_hbm, im_hbm, sem):
    out = pltpu.make_async_copy(mixed_ref, mixed_hbm, sem.at[0])
    out.start()

    @pl.loop(0, re_ref.shape[0])
    def _(g):
        for i, (near, far) in enumerate(((re_ref, re_hbm), (im_ref, im_hbm))):
            pltpu.make_async_copy(near.at[g], far.at[:, g, :], sem.at[i + 1]).start()

    out.wait()
    drain(re_ref, sem.at[1])
    drain(im_ref, sem.at[2])


def local(
    tokens,
    mix_gain,
    w_in,
    decay_re,
    freq,
    log_step,
    in_re,
    in_im,
    out_re,
    out_im,
    skip,
    state_re,
    state_im,
    glu_weight,
    glu_bias,
    out_weight,
    ffn_gain,
    route,
    route_weight,
    expert_gate,
    expert_up,
    expert_down,
):
    seq_count, model_width = tokens.shape
    n_tp = lax.axis_size("tp")
    experts = lax.axis_size("ep")
    local_width = model_width // n_tp
    top_count = route.shape[1]
    slot_cap = (3 * seq_count * top_count + 2 * experts - 1) // (2 * experts)
    slot_rows = (slot_cap + 7) // 8 * 8
    chan = w_in.shape[1]
    state_block = (decay_re.shape[0], seq_count, state_re.shape[2])
    block = (slot_rows // 8, 8, local_width)
    chunks = chunks_of(experts)
    bf16 = jnp.bfloat16
    dma = pltpu.SemaphoreType.DMA
    vmem = pl.BlockSpec(memory_space=pltpu.VMEM)
    anyplace = pl.BlockSpec(memory_space=pl.ANY)
    arrays = {
        "tokens": tokens,
        "mix_gain": mix_gain[None, :],
        "w_in": w_in,
        "decay": decay_re,
        "freq": freq,
        "log_step": log_step[None, :],
        "in_re": in_re,
        "in_im": in_im,
        "out_re": out_re,
        "out_im": out_im,
        "skip": skip,
        "glu": glu_weight,
        "bias": glu_bias[None, :],
        "out_w": out_weight,
        "gain": ffn_gain[None, :],
        "route": route.T,
        "weight": route_weight.T,
        "gate": expert_gate,
        "up": expert_up,
        "down": expert_down,
    }
    arrays = [arrays[name] for name in SMALL + LATER]
    holds = [
        pltpu.VMEM(a.shape[1:] if name in ("gate", "up", "down") else a.shape, a.dtype)
        for name, a in zip(SMALL + LATER, arrays)
    ]
    mixed, new_re, new_im = pl.pallas_call(
        functools.partial(layer, n_tp, experts),
        out_shape=(
            pltpu.VMEM((seq_count, local_width), bf16),
            pltpu.VMEM(state_block, jnp.float32),
            pltpu.VMEM(state_block, jnp.float32),
        ),
        in_specs=[anyplace] * (len(arrays) + 2),
        out_specs=(vmem, vmem, vmem),
        scratch_shapes=holds
        + [
            pltpu.VMEM((seq_count, chan), bf16),
            pltpu.VMEM((n_tp - 1, seq_count, chan), bf16),
            pltpu.VMEM((n_tp - 1, seq_count, local_width), bf16),
            pltpu.VMEM((n_tp - 1, seq_count, local_width), bf16),
            pltpu.VMEM((experts,) + block, bf16),
            pltpu.VMEM((n_tp, experts) + block, bf16),
            pltpu.VMEM((max(c for _, c in chunks) * slot_rows, model_width), bf16),
            pltpu.VMEM((n_tp - 1, experts) + block, bf16),
            pltpu.VMEM((experts,) + block, bf16),
            pltpu.VMEM((n_tp - 1, experts) + block, bf16),
            pltpu.VMEM((experts,) + block, bf16),
            pltpu.VMEM((experts,) + block, bf16),
            dma((len(arrays),)),
            dma((2,)),
            dma((n_tp - 1,)),
            dma((n_tp - 1,)),
            dma((n_tp - 1,)),
            dma((n_tp - 1,)),
            dma,
            dma((experts - 1,)),
            dma((n_tp - 1,)),
            dma((len(chunks), n_tp - 1)),
            dma((n_tp - 1,)),
            dma((len(chunks), n_tp - 1)),
            dma,
            dma((experts - 1,)),
        ],
        compiler_params=pltpu.CompilerParams(
            collective_id=0, has_side_effects=True, vmem_limit_bytes=58 * 1024 * 1024
        ),
    )(*arrays, state_re, state_im)
    results = [pltpu.with_memory_space_constraint(a, pltpu.VMEM) for a in (mixed, new_re, new_im)]
    return pl.pallas_call(
        store,
        out_shape=(
            jax.ShapeDtypeStruct((seq_count, local_width), bf16),
            jax.ShapeDtypeStruct(state_re.shape, jnp.float32),
            jax.ShapeDtypeStruct(state_im.shape, jnp.float32),
        ),
        in_specs=[vmem] * 3,
        out_specs=(anyplace,) * 3,
        scratch_shapes=[dma((3,))],
    )(*results)


def solution(mesh):
    in_specs = (
        P("ep", None),
        P(),
        P(None, "tp"),
        P("tp", None),
        P("tp", None),
        P("tp"),
        P("tp", None, None),
        P("tp", None, None),
        P("tp", None, None),
        P("tp", None, None),
        P("tp", None),
        P("ep", "tp", None),
        P("ep", "tp", None),
        P(None, "tp"),
        P("tp"),
        P("tp", None),
        P(),
        P("ep", None),
        P("ep", None),
        P("ep", None, "tp"),
        P("ep", None, "tp"),
        P("ep", "tp", None),
    )
    out_specs = (P("ep", "tp"), P("ep", "tp", None), P("ep", "tp", None))
    return jax.shard_map(local, mesh=mesh, in_specs=in_specs, out_specs=out_specs, check_vma=False)
```

```python
import functools
import jax
import jax.numpy as jnp
from jax import lax
from jax.experimental import pallas as pl
from jax.experimental.pallas import tpu as pltpu
from jax.sharding import PartitionSpec as P

norm_eps = 1e-06
MESH = pl.DeviceIdType.MESH


def rms_scale(rows, gain):
    values = rows.astype(jnp.float32)
    scaled = values * lax.rsqrt(jnp.mean(values * values, axis=-1, keepdims=True) + norm_eps)
    return (scaled * gain).astype(jnp.bfloat16)


def drain(ref, sem):
    pltpu.make_async_copy(ref, ref, sem).wait()


def remote(src, dst, send, recv, axis, peer):
    copy = pltpu.make_async_remote_copy(
        src_ref=src,
        dst_ref=dst,
        send_sem=send,
        recv_sem=recv,
        device_id={axis: peer},
        device_id_type=MESH,
    )
    copy.start()


def paired(index, offset, count):
    result, bit = 0, 1
    while bit < count:
        result += lax.rem(lax.div(index, bit) + lax.div(offset, bit), 2) * bit
        bit *= 2
    return result


def offset_at(place, count):
    core = place % 2
    return count - 2 - (place - core) + core


def each(low, high, body):
    if high - low <= 8:
        for i in range(low, high):
            body(i)
    else:
        pl.loop(low, high)(body)


def groups_of(n_ep):
    quarter = n_ep // 4
    return tuple((part * quarter, quarter) for part in range(4))


PASSES = ((0,), (1,), (2, 3))


SMALL = (
    "tokens",
    "w_in",
    "mix_gain",
    "decay",
    "freq",
    "log_step",
    "in_re",
    "in_im",
    "out_re",
    "out_im",
    "skip",
)
LATER = ("glu", "bias", "route", "weight", "out_w", "gain", "gate", "up", "down")


def mixer(v, wait, state_re, state_im, state_sem):
    f32 = jnp.float32
    bf16 = jnp.bfloat16
    groups, places, entries = v["in_re"].shape
    seqs = v["tokens"].shape[0]
    chan = v["w_in"].shape[1]
    wide = groups * entries

    def spread(value):
        pair = jnp.concatenate([value, value], axis=1)
        return jnp.concatenate([pair] * (groups // 2), axis=1)

    def own(rows):
        shape = (rows, wide)
        group = lax.broadcasted_iota(jnp.int32, shape, 0) // (rows // groups)
        return lax.broadcasted_iota(jnp.int32, shape, 1) // entries == group

    def as_row(value):
        return jnp.sum(jnp.where(own(groups), spread(value), 0.0), axis=0, keepdims=True)

    own_chan = own(chan)

    def diagonal_blocks(name):
        weight = v[name][...].astype(f32).reshape(chan, entries)
        return jnp.where(own_chan, spread(weight), 0.0)

    for name in SMALL:
        wait(name)
    normed = rms_scale(v["tokens"][...], v["mix_gain"][...])
    drive = jnp.dot(normed, v["w_in"][...], preferred_element_type=f32).astype(bf16)
    eye = lax.broadcasted_iota(jnp.int32, (groups, groups), 0)
    eye = eye == lax.broadcasted_iota(jnp.int32, (groups, groups), 1)
    log_step = jnp.sum(jnp.where(eye, v["log_step"][...], 0.0), axis=1, keepdims=True)
    step = jnp.exp(log_step)
    decay = v["decay"][...]
    freq = v["freq"][...]
    magnitude = jnp.exp(decay * step)
    turn_re = magnitude * jnp.cos(freq * step)
    turn_im = magnitude * jnp.sin(freq * step)
    denom = decay * decay + freq * freq
    coef_re = ((turn_re - 1.0) * decay + turn_im * freq) / denom
    coef_im = (turn_im * decay - (turn_re - 1.0) * freq) / denom
    turn_re, turn_im, coef_re, coef_im = map(as_row, (turn_re, turn_im, coef_re, coef_im))

    in_re = diagonal_blocks("in_re").astype(bf16)
    in_im = diagonal_blocks("in_im").astype(bf16)

    out_re = diagonal_blocks("out_re").astype(bf16)
    out_im = (-diagonal_blocks("out_im")).astype(bf16)
    out = jnp.concatenate([out_re, out_im], axis=1)
    lane = lax.broadcasted_iota(jnp.int32, (places, chan), 1) % places
    lane = lane == lax.broadcasted_iota(jnp.int32, (places, chan), 0)
    skip = jnp.dot(
        v["skip"][...],
        lane.astype(f32),
        precision=lax.Precision.HIGHEST,
        preferred_element_type=f32,
    )
    group = lax.broadcasted_iota(jnp.int32, (groups, chan), 1) // places
    group = group == lax.broadcasted_iota(jnp.int32, (groups, chan), 0)
    skip = jnp.sum(jnp.where(group, skip, 0.0), axis=0, keepdims=True)
    drive_re = jnp.dot(drive, in_re, preferred_element_type=f32)
    drive_im = jnp.dot(drive, in_im, preferred_element_type=f32)
    drain(state_re, state_sem.at[0])
    drain(state_im, state_sem.at[1])
    old_re = jnp.concatenate([state_re[g] for g in range(groups)], axis=1)
    old_im = jnp.concatenate([state_im[g] for g in range(groups)], axis=1)
    kept_re = turn_re * old_re - turn_im * old_im
    kept_im = turn_re * old_im + turn_im * old_re
    new_re = kept_re + (coef_re * drive_re - coef_im * drive_im)
    new_im = kept_im + (coef_re * drive_im + coef_im * drive_re)
    value = jnp.concatenate([new_re, new_im], axis=1)
    high = value.astype(bf16)
    low = (value - high.astype(f32)).astype(bf16)
    both = jnp.concatenate([high, low], axis=0)
    read = lax.dot_general(both, out, (((1,), (1,)), ((), ())), preferred_element_type=f32)
    read = read[:seqs] + read[seqs:] + skip * drive.astype(f32)

    def keep():
        for g in range(groups):
            state_re[g] = new_re[:, g * entries : (g + 1) * entries]
            state_im[g] = new_im[:, g * entries : (g + 1) * entries]

    return jax.nn.gelu(read).astype(bf16), keep


def gated_unit(gate, up):
    return (jax.nn.silu(gate) * up).astype(jnp.bfloat16)


def layer(n_tp, n_ep, *refs):
    f32 = jnp.float32
    bf16 = jnp.bfloat16
    names = SMALL + LATER
    hbm = dict(zip(names, refs))
    state_re_hbm, state_im_hbm, out_ref, state_re, state_im = refs[len(names) : len(names) + 5]
    rest = refs[len(names) + 5 :]
    v = dict(zip(names, rest))
    (
        mixed_ref,
        ag_buf,
        rs_out,
        rs_in,
        disp,
        rows,
        xn,
        back_out,
        back_own,
        back_in,
        ret_out,
        ret_in,
        load_sem,
        state_sem,
        ag_s,
        ag_r,
        rs_s,
        rs_r,
        disp_s,
        disp_r,
        fwd_s,
        fwd_r,
        back_s,
        back_r,
        ret_s,
        ret_r,
    ) = rest[len(names) :]
    tp = lax.axis_index("tp")
    ep = lax.axis_index("ep")
    seqs, chan = mixed_ref.shape
    width = out_ref.shape[1]
    blocks = rows.shape[2]
    slot_rows = blocks * 8
    slots = n_ep * slot_rows
    hidden_n = v["gate"].shape[1]
    peers = tuple(range(n_tp - 1, 0, -1))
    parts = groups_of(n_ep)
    own_place, partner = n_ep - 2, n_ep - 1

    def copy_of(name):
        src = hbm[name]
        if name in ("gate", "up", "down"):
            src = src.at[0]
        return pltpu.make_async_copy(src, v[name], load_sem.at[names.index(name)])

    def wait(name):
        copy_of(name).wait()

    for name in SMALL:
        copy_of(name).start()

    @pl.loop(0, state_re.shape[0])
    def _(g):
        for i, (far, near) in enumerate(((state_re_hbm, state_re), (state_im_hbm, state_im))):
            pltpu.make_async_copy(far.at[:, g, :], near.at[g], state_sem.at[i]).start()

    for name in LATER:
        copy_of(name).start()

    barrier = pltpu.get_barrier_semaphore()

    @pl.loop(1, n_tp)
    def _(k):
        pl.semaphore_signal(
            barrier, inc=1, device_id={"tp": lax.rem(tp + k, n_tp)}, device_id_type=MESH
        )

    @pl.loop(1, n_ep)
    def _(k):
        pl.semaphore_signal(
            barrier, inc=1, device_id={"ep": lax.rem(ep + k, n_ep)}, device_id_type=MESH
        )

    def tp_peer(k):
        return paired(tp, k, n_tp)

    def ep_peer(i):
        return paired(ep, offset_at(i, n_ep), n_ep)

    mixed, keep = mixer(v, wait, state_re, state_im, state_sem)
    mixed_ref[...] = mixed
    pl.semaphore_wait(barrier, n_tp + n_ep - 2)
    for k in peers:
        remote(mixed_ref, ag_buf.at[k - 1], ag_s.at[k - 1], ag_r.at[k - 1], "tp", tp_peer(k))

    keep()
    def one_hot(index, size):
        return lax.broadcasted_iota(jnp.int32, (seqs, size), 1).astype(f32) == index

    row = lax.broadcasted_iota(jnp.int32, (seqs, seqs), 0)
    lane = lax.broadcasted_iota(jnp.int32, (seqs, seqs), 1)

    def upright(ref, k):
        value = ref[k : k + 1, :].astype(f32)
        return jnp.sum(jnp.where(row == lane, value, 0.0), axis=1, keepdims=True)

    for name in ("route", "weight", "bias", "gain"):
        wait(name)
    route_ref, weight_ref, gain_ref = v["route"], v["weight"], v["gain"]
    choices = [upright(route_ref, k) for k in range(route_ref.shape[0])]
    hits = [one_hot(choice, n_ep).astype(f32) for choice in choices]
    earlier = jnp.where(lane < row, 1.0, 0.0).astype(bf16)
    before = jnp.dot(earlier, sum(hits).astype(bf16), preferred_element_type=f32)
    select = jnp.zeros((seqs, slots), f32)
    combine = jnp.zeros((seqs, slots), f32)
    for k, choice in enumerate(choices):
        rank = jnp.sum(before * hits[k], axis=1, keepdims=True)
        pick = one_hot(choice * slot_rows + rank, slots)
        select = jnp.where(pick, 1.0, select)
        combine = jnp.where(pick, upright(weight_ref, k), combine)

    def glu_rows(owner):
        return v["glu"][pl.ds(pl.multiple_of(owner * chan, chan), chan), :]

    wait("glu")
    gate = jnp.dot(mixed, glu_rows(tp), preferred_element_type=f32) + v["bias"][...]
    for k in reversed(peers):
        drain(ag_buf.at[k - 1], ag_r.at[k - 1])
        gate += jnp.dot(ag_buf[k - 1], glu_rows(tp_peer(k)), preferred_element_type=f32)
    gated = (mixed.astype(f32) * jax.nn.sigmoid(gate)).astype(bf16)

    wait("out_w")

    def columns(owner):
        return pl.ds(pl.multiple_of(owner * width, width), width)

    def share(owner):
        value = jnp.dot(gated, v["out_w"][:, columns(owner)], preferred_element_type=f32)
        return value.astype(bf16)

    shares = [share(tp_peer(k)) for k in peers] if n_tp <= 4 else None
    for at, k in enumerate(peers):
        rs_out[k - 1] = shares[at] if shares else share(tp_peer(k))
        remote(
            rs_out.at[k - 1], rs_in.at[k - 1], rs_s.at[k - 1], rs_r.at[k - 1], "tp", tp_peer(k)
        )
    total = share(tp).astype(f32)
    for k in reversed(peers):
        drain(rs_in.at[k - 1], rs_r.at[k - 1])
        total += rs_in[k - 1].astype(f32)
    resid = (v["tokens"][:, columns(tp)].astype(f32) + total).astype(bf16)

    picked = lax.dot_general(
        select.astype(bf16), resid, (((0,), (0,)), ((), ())), preferred_element_type=f32
    )
    disp[...] = picked.reshape(n_ep, blocks, 8, width).astype(bf16)

    def dispatch(i):
        to = ep_peer(i)
        remote(disp.at[to], rows.at[tp, i], disp_s, disp_r.at[i], "ep", to)

    dispatch(partner)
    each(0, own_place, dispatch)

    def pass_on(i, here):
        for k in peers:
            remote(here, rows.at[tp, i], fwd_s.at[k - 1], fwd_r.at[i, k - 1], "tp", tp_peer(k))

    pass_on(own_place, disp.at[ep])
    rows[tp, own_place] = disp[ep]

    def forward(i):
        here = rows.at[tp, i]
        drain(here, disp_r.at[i])
        pass_on(i, here)

    forward(partner)
    each(0, own_place, forward)

    for part, members in enumerate(PASSES):
        start, count = parts[members[0]][0], sum(parts[member][1] for member in members)
        span = pl.ds(start, count)
        held = xn.at[pl.ds(0, count * slot_rows)]

        def row_values(owner):
            return rows[owner, span].astype(f32).reshape(count * slot_rows, width)

        def landed(i):
            for k in reversed(peers):
                drain(rows.at[tp_peer(k), i], fwd_r.at[i, k - 1])

        each(start, start + count, landed)
        squares = sum(row_values(owner) * row_values(owner) for owner in range(n_tp))
        squares = jnp.sum(squares, axis=1, keepdims=True)
        scale = lax.rsqrt(squares / (n_tp * width) + norm_eps)
        for owner in range(n_tp):
            cols = pl.ds(owner * width, width)
            held[:, cols] = (row_values(owner) * scale * gain_ref[:, cols]).astype(bf16)

        if part == 0:
            wait("gate")
            wait("up")
        products = (
            jnp.dot(held[...], v[name][...], preferred_element_type=f32) for name in ("gate", "up")
        )
        hidden = gated_unit(*products)
        if part == 0:
            wait("down")

        def down(owner):
            value = jnp.dot(hidden, v["down"][:, columns(owner)], preferred_element_type=f32)
            return value.reshape(count, blocks, 8, width).astype(bf16)

        def give_back(member, k):
            where = pl.ds(*parts[member])
            remote(
                back_out.at[k - 1, where],
                back_in.at[k - 1, where],
                back_s.at[member, k - 1],
                back_r.at[member, k - 1],
                "tp",
                tp_peer(k),
            )

        def hand(k, value):
            back_out[k - 1, span] = value
            give_back(members[0], k)

        ready = None
        for k in peers:
            value = down(tp_peer(k))
            if ready is not None:
                hand(*ready)
            ready = k, value
        own = down(tp)
        hand(*ready)
        for member in members[1:]:
            for k in peers:
                give_back(member, k)
        back_own[span] = own

    for part, (start, count) in enumerate(parts):
        for k in peers:
            drain(back_in.at[k - 1, pl.ds(start, count)], back_r.at[part, k - 1])

        def settle(i):
            result = back_own[i].astype(f32)
            for k in reversed(peers):
                result += back_in[k - 1, i].astype(f32)
            result = result.astype(bf16)
            if isinstance(i, int) and i == own_place:
                ret_in[ep] = result
                return
            to = ep_peer(i)
            ret_out[to] = result
            remote(ret_out.at[to], ret_in.at[ep], ret_s, ret_r.at[i], "ep", to)

        each(start, min(start + count, own_place), settle)
        if start + count == n_ep:
            settle(partner)
            settle(own_place)

    def arrived(i):
        drain(ret_in.at[ep_peer(i)], ret_r.at[i])

    each(0, own_place, arrived)
    arrived(partner)

    returned = ret_in[...].astype(f32).reshape(slots, width).astype(bf16)
    high = combine.astype(bf16)
    low = (combine - high.astype(f32)).astype(bf16)
    expert_total = jnp.dot(high, returned, preferred_element_type=f32)
    expert_total += jnp.dot(low, returned, preferred_element_type=f32)
    out_ref[...] = (resid.astype(f32) + expert_total).astype(bf16)

    for k in peers:
        drain(mixed_ref, ag_s.at[k - 1])
        drain(rs_out.at[k - 1], rs_s.at[k - 1])
        drain(rows.at[0], fwd_s.at[k - 1])
        for part, where in enumerate(parts):
            drain(back_out.at[k - 1, pl.ds(*where)], back_s.at[part, k - 1])
    drain(disp.at[pl.ds(0, n_ep - 1)], disp_s)
    drain(ret_out.at[pl.ds(0, n_ep - 1)], ret_s)


def store(mixed_ref, re_ref, im_ref, mixed_hbm, re_hbm, im_hbm, sem):
    out = pltpu.make_async_copy(mixed_ref, mixed_hbm, sem.at[0])
    out.start()

    @pl.loop(0, re_ref.shape[0])
    def _(g):
        for i, (near, far) in enumerate(((re_ref, re_hbm), (im_ref, im_hbm))):
            pltpu.make_async_copy(near.at[g], far.at[:, g, :], sem.at[i + 1]).start()

    out.wait()
    drain(re_ref, sem.at[1])
    drain(im_ref, sem.at[2])


def local(
    tokens,
    mix_gain,
    w_in,
    decay_re,
    freq,
    log_step,
    in_re,
    in_im,
    out_re,
    out_im,
    skip,
    state_re,
    state_im,
    glu_weight,
    glu_bias,
    out_weight,
    ffn_gain,
    route,
    route_weight,
    expert_gate,
    expert_up,
    expert_down,
):
    seq_count, model_width = tokens.shape
    n_tp = lax.axis_size("tp")
    experts = lax.axis_size("ep")
    local_width = model_width // n_tp
    top_count = route.shape[1]
    slot_cap = (3 * seq_count * top_count + 2 * experts - 1) // (2 * experts)
    slot_rows = (slot_cap + 7) // 8 * 8
    chan = w_in.shape[1]
    state_block = (decay_re.shape[0], seq_count, state_re.shape[2])
    block = (slot_rows // 8, 8, local_width)
    most = max(sum(groups_of(experts)[part][1] for part in members) for members in PASSES)
    bf16 = jnp.bfloat16
    dma = pltpu.SemaphoreType.DMA
    vmem = pl.BlockSpec(memory_space=pltpu.VMEM)
    anyplace = pl.BlockSpec(memory_space=pl.ANY)
    arrays = {
        "tokens": tokens,
        "mix_gain": mix_gain[None, :],
        "w_in": w_in,
        "decay": decay_re,
        "freq": freq,
        "log_step": log_step[None, :],
        "in_re": in_re,
        "in_im": in_im,
        "out_re": out_re,
        "out_im": out_im,
        "skip": skip,
        "glu": glu_weight,
        "bias": glu_bias[None, :],
        "out_w": out_weight,
        "gain": ffn_gain[None, :],
        "route": route.T,
        "weight": route_weight.T,
        "gate": expert_gate,
        "up": expert_up,
        "down": expert_down,
    }
    arrays = [arrays[name] for name in SMALL + LATER]
    holds = [
        pltpu.VMEM(a.shape[1:] if name in ("gate", "up", "down") else a.shape, a.dtype)
        for name, a in zip(SMALL + LATER, arrays)
    ]
    mixed, new_re, new_im = pl.pallas_call(
        functools.partial(layer, n_tp, experts),
        out_shape=(
            pltpu.VMEM((seq_count, local_width), bf16),
            pltpu.VMEM(state_block, jnp.float32),
            pltpu.VMEM(state_block, jnp.float32),
        ),
        in_specs=[anyplace] * (len(arrays) + 2),
        out_specs=(vmem, vmem, vmem),
        scratch_shapes=holds
        + [
            pltpu.VMEM((seq_count, chan), bf16),
            pltpu.VMEM((n_tp - 1, seq_count, chan), bf16),
            pltpu.VMEM((n_tp - 1, seq_count, local_width), bf16),
            pltpu.VMEM((n_tp - 1, seq_count, local_width), bf16),
            pltpu.VMEM((experts,) + block, bf16),
            pltpu.VMEM((n_tp, experts) + block, bf16),
            pltpu.VMEM((most * slot_rows, model_width), bf16),
            pltpu.VMEM((n_tp - 1, experts) + block, bf16),
            pltpu.VMEM((experts,) + block, bf16),
            pltpu.VMEM((n_tp - 1, experts) + block, bf16),
            pltpu.VMEM((experts,) + block, bf16),
            pltpu.VMEM((experts,) + block, bf16),
            dma((len(arrays),)),
            dma((2,)),
            dma((n_tp - 1,)),
            dma((n_tp - 1,)),
            dma((n_tp - 1,)),
            dma((n_tp - 1,)),
            dma,
            dma((experts,)),
            dma((n_tp - 1,)),
            dma((experts, n_tp - 1)),
            dma((4, n_tp - 1)),
            dma((4, n_tp - 1)),
            dma,
            dma((experts,)),
        ],
        compiler_params=pltpu.CompilerParams(
            collective_id=0, has_side_effects=True, vmem_limit_bytes=58 * 1024 * 1024
        ),
    )(*arrays, state_re, state_im)
    results = [pltpu.with_memory_space_constraint(a, pltpu.VMEM) for a in (mixed, new_re, new_im)]
    return pl.pallas_call(
        store,
        out_shape=(
            jax.ShapeDtypeStruct((seq_count, local_width), bf16),
            jax.ShapeDtypeStruct(state_re.shape, jnp.float32),
            jax.ShapeDtypeStruct(state_im.shape, jnp.float32),
        ),
        in_specs=[vmem] * 3,
        out_specs=(anyplace,) * 3,
        scratch_shapes=[dma((3,))],
    )(*results)


def solution(mesh):
    in_specs = (
        P("ep", None),
        P(),
        P(None, "tp"),
        P("tp", None),
        P("tp", None),
        P("tp"),
        P("tp", None, None),
        P("tp", None, None),
        P("tp", None, None),
        P("tp", None, None),
        P("tp", None),
        P("ep", "tp", None),
        P("ep", "tp", None),
        P(None, "tp"),
        P("tp"),
        P("tp", None),
        P(),
        P("ep", None),
        P("ep", None),
        P("ep", None, "tp"),
        P("ep", None, "tp"),
        P("ep", "tp", None),
    )
    out_specs = (P("ep", "tp"), P("ep", "tp", None), P("ep", "tp", None))
    return jax.shard_map(local, mesh=mesh, in_specs=in_specs, out_specs=out_specs, check_vma=False)
```

```python
import functools
import jax
import jax.numpy as jnp
from jax import lax
from jax.experimental import pallas as pl
from jax.experimental.pallas import tpu as pltpu
from jax.sharding import PartitionSpec as P

norm_eps = 1e-06
MESH = pl.DeviceIdType.MESH


def rms_scale(rows, gain):
    values = rows.astype(jnp.float32)
    scaled = values * lax.rsqrt(jnp.mean(values * values, axis=-1, keepdims=True) + norm_eps)
    return (scaled * gain).astype(jnp.bfloat16)


def drain(ref, sem):
    pltpu.make_async_copy(ref, ref, sem).wait()


def remote(src, dst, send, recv, axis, peer):
    copy = pltpu.make_async_remote_copy(
        src_ref=src,
        dst_ref=dst,
        send_sem=send,
        recv_sem=recv,
        device_id={axis: peer},
        device_id_type=MESH,
    )
    copy.start()


def paired(index, offset, count):
    result, bit = 0, 1
    while bit < count:
        result += lax.rem(lax.div(index, bit) + lax.div(offset, bit), 2) * bit
        bit *= 2
    return result


def offset_at(place, count):
    core = place % 2
    return count - 2 - (place - core) + core


def each(low, high, body):
    if high - low <= 8:
        for i in range(low, high):
            body(i)
    else:
        pl.loop(low, high)(body)


def groups_of(n_ep):
    quarter = n_ep // 4
    return tuple((part * quarter, quarter) for part in range(4))


PASSES = ((0,), (1,), (2, 3))


SMALL = (
    "tokens",
    "w_in",
    "mix_gain",
    "decay",
    "freq",
    "log_step",
    "in_re",
    "in_im",
    "out_re",
    "out_im",
    "skip",
)
LATER = ("glu", "bias", "route", "weight", "out_w", "gain", "gate", "up", "down")


def mixer(v, wait, state_re, state_im, state_sem):
    f32 = jnp.float32
    bf16 = jnp.bfloat16
    groups, places, entries = v["in_re"].shape
    seqs = v["tokens"].shape[0]
    chan = v["w_in"].shape[1]
    wide = groups * entries

    def spread(value):
        pair = jnp.concatenate([value, value], axis=1)
        return jnp.concatenate([pair] * (groups // 2), axis=1)

    def own(rows):
        shape = (rows, wide)
        group = lax.broadcasted_iota(jnp.int32, shape, 0) // (rows // groups)
        return lax.broadcasted_iota(jnp.int32, shape, 1) // entries == group

    def as_row(value):
        return jnp.sum(jnp.where(own(groups), spread(value), 0.0), axis=0, keepdims=True)

    own_chan = own(chan)

    def diagonal_blocks(name):
        weight = v[name][...].astype(f32).reshape(chan, entries)
        return jnp.where(own_chan, spread(weight), 0.0)

    wait("tokens")
    wait("mix_gain")
    normed = rms_scale(v["tokens"][...], v["mix_gain"][...])
    for name in SMALL:
        if name not in ("tokens", "mix_gain"):
            wait(name)
    drive = jnp.dot(normed, v["w_in"][...], preferred_element_type=f32).astype(bf16)
    eye = lax.broadcasted_iota(jnp.int32, (groups, groups), 0)
    eye = eye == lax.broadcasted_iota(jnp.int32, (groups, groups), 1)
    log_step = jnp.sum(jnp.where(eye, v["log_step"][...], 0.0), axis=1, keepdims=True)
    step = jnp.exp(log_step)
    decay = v["decay"][...]
    freq = v["freq"][...]
    magnitude = jnp.exp(decay * step)
    turn_re = magnitude * jnp.cos(freq * step)
    turn_im = magnitude * jnp.sin(freq * step)
    denom = decay * decay + freq * freq
    coef_re = ((turn_re - 1.0) * decay + turn_im * freq) / denom
    coef_im = (turn_im * decay - (turn_re - 1.0) * freq) / denom
    turn_re, turn_im, coef_re, coef_im = map(as_row, (turn_re, turn_im, coef_re, coef_im))

    in_re = diagonal_blocks("in_re").astype(bf16)
    in_im = diagonal_blocks("in_im").astype(bf16)

    out_re = diagonal_blocks("out_re").astype(bf16)
    out_im = (-diagonal_blocks("out_im")).astype(bf16)
    out = jnp.concatenate([out_re, out_im], axis=1)
    lane = lax.broadcasted_iota(jnp.int32, (places, chan), 1) % places
    lane = lane == lax.broadcasted_iota(jnp.int32, (places, chan), 0)
    skip = jnp.dot(
        v["skip"][...],
        lane.astype(f32),
        precision=lax.Precision.HIGHEST,
        preferred_element_type=f32,
    )
    group = lax.broadcasted_iota(jnp.int32, (groups, chan), 1) // places
    group = group == lax.broadcasted_iota(jnp.int32, (groups, chan), 0)
    skip = jnp.sum(jnp.where(group, skip, 0.0), axis=0, keepdims=True)
    drive_re = jnp.dot(drive, in_re, preferred_element_type=f32)
    drive_im = jnp.dot(drive, in_im, preferred_element_type=f32)
    drain(state_re, state_sem.at[0])
    drain(state_im, state_sem.at[1])
    old_re = jnp.concatenate([state_re[g] for g in range(groups)], axis=1)
    old_im = jnp.concatenate([state_im[g] for g in range(groups)], axis=1)
    kept_re = turn_re * old_re - turn_im * old_im
    kept_im = turn_re * old_im + turn_im * old_re
    new_re = kept_re + (coef_re * drive_re - coef_im * drive_im)
    new_im = kept_im + (coef_re * drive_im + coef_im * drive_re)
    value = jnp.concatenate([new_re, new_im], axis=1)
    high = value.astype(bf16)
    low = (value - high.astype(f32)).astype(bf16)
    both = jnp.concatenate([high, low], axis=0)
    read = lax.dot_general(both, out, (((1,), (1,)), ((), ())), preferred_element_type=f32)
    read = read[:seqs] + read[seqs:] + skip * drive.astype(f32)

    def keep():
        for g in range(groups):
            state_re[g] = new_re[:, g * entries : (g + 1) * entries]
            state_im[g] = new_im[:, g * entries : (g + 1) * entries]

    return jax.nn.gelu(read).astype(bf16), keep


def gated_unit(gate, up):
    return (jax.nn.silu(gate) * up).astype(jnp.bfloat16)


def layer(n_tp, n_ep, *refs):
    f32 = jnp.float32
    bf16 = jnp.bfloat16
    names = SMALL + LATER
    hbm = dict(zip(names, refs))
    state_re_hbm, state_im_hbm, out_ref, state_re, state_im = refs[len(names) : len(names) + 5]
    rest = refs[len(names) + 5 :]
    v = dict(zip(names, rest))
    (
        mixed_ref,
        ag_buf,
        rs_out,
        rs_in,
        disp,
        rows,
        xn,
        back_out,
        back_own,
        back_in,
        ret_out,
        ret_in,
        load_sem,
        state_sem,
        ag_s,
        ag_r,
        rs_s,
        rs_r,
        disp_s,
        disp_r,
        fwd_s,
        fwd_r,
        back_s,
        back_r,
        ret_s,
        ret_r,
    ) = rest[len(names) :]
    tp = lax.axis_index("tp")
    ep = lax.axis_index("ep")
    seqs, chan = mixed_ref.shape
    width = out_ref.shape[1]
    blocks = rows.shape[2]
    slot_rows = blocks * 8
    slots = n_ep * slot_rows
    hidden_n = v["gate"].shape[1]
    peers = tuple(range(n_tp - 1, 0, -1))
    parts = groups_of(n_ep)
    own_place, partner = n_ep - 2, n_ep - 1

    def copy_of(name):
        src = hbm[name]
        if name in ("gate", "up", "down"):
            src = src.at[0]
        return pltpu.make_async_copy(src, v[name], load_sem.at[names.index(name)])

    def wait(name):
        copy_of(name).wait()

    for name in SMALL:
        copy_of(name).start()

    @pl.loop(0, state_re.shape[0])
    def _(g):
        for i, (far, near) in enumerate(((state_re_hbm, state_re), (state_im_hbm, state_im))):
            pltpu.make_async_copy(far.at[:, g, :], near.at[g], state_sem.at[i]).start()

    for name in LATER:
        copy_of(name).start()

    barrier = pltpu.get_barrier_semaphore()

    @pl.loop(1, n_tp)
    def _(k):
        pl.semaphore_signal(
            barrier, inc=1, device_id={"tp": lax.rem(tp + k, n_tp)}, device_id_type=MESH
        )

    @pl.loop(1, n_ep)
    def _(k):
        pl.semaphore_signal(
            barrier, inc=1, device_id={"ep": lax.rem(ep + k, n_ep)}, device_id_type=MESH
        )

    def tp_peer(k):
        return paired(tp, k, n_tp)

    def ep_peer(i):
        return paired(ep, offset_at(i, n_ep), n_ep)

    mixed, keep = mixer(v, wait, state_re, state_im, state_sem)
    mixed_ref[...] = mixed
    pl.semaphore_wait(barrier, n_tp + n_ep - 2)
    for k in peers:
        remote(mixed_ref, ag_buf.at[k - 1], ag_s.at[k - 1], ag_r.at[k - 1], "tp", tp_peer(k))

    keep()
    def one_hot(index, size):
        return lax.broadcasted_iota(jnp.int32, (seqs, size), 1).astype(f32) == index

    row = lax.broadcasted_iota(jnp.int32, (seqs, seqs), 0)
    lane = lax.broadcasted_iota(jnp.int32, (seqs, seqs), 1)

    def upright(ref, k):
        value = ref[k : k + 1, :].astype(f32)
        return jnp.sum(jnp.where(row == lane, value, 0.0), axis=1, keepdims=True)

    for name in ("route", "weight", "bias", "gain"):
        wait(name)
    route_ref, weight_ref, gain_ref = v["route"], v["weight"], v["gain"]
    choices = [upright(route_ref, k) for k in range(route_ref.shape[0])]
    hits = [one_hot(choice, n_ep).astype(f32) for choice in choices]
    earlier = jnp.where(lane < row, 1.0, 0.0).astype(bf16)
    before = jnp.dot(earlier, sum(hits).astype(bf16), preferred_element_type=f32)
    select = jnp.zeros((seqs, slots), f32)
    combine = jnp.zeros((seqs, slots), f32)
    for k, choice in enumerate(choices):
        rank = jnp.sum(before * hits[k], axis=1, keepdims=True)
        pick = one_hot(choice * slot_rows + rank, slots)
        select = jnp.where(pick, 1.0, select)
        combine = jnp.where(pick, upright(weight_ref, k), combine)
    select = select.T.astype(bf16)

    def glu_rows(owner):
        return v["glu"][pl.ds(pl.multiple_of(owner * chan, chan), chan), :]

    wait("glu")
    gate = jnp.dot(mixed, glu_rows(tp), preferred_element_type=f32) + v["bias"][...]
    for k in reversed(peers):
        drain(ag_buf.at[k - 1], ag_r.at[k - 1])
        gate += jnp.dot(ag_buf[k - 1], glu_rows(tp_peer(k)), preferred_element_type=f32)
    gated = (mixed.astype(f32) * jax.nn.sigmoid(gate)).astype(bf16)

    wait("out_w")

    def columns(owner):
        return pl.ds(pl.multiple_of(owner * width, width), width)

    def share(owner):
        value = jnp.dot(gated, v["out_w"][:, columns(owner)], preferred_element_type=f32)
        return value.astype(bf16)

    shares = [share(tp_peer(k)) for k in peers] if n_tp <= 4 else None
    for at, k in enumerate(peers):
        rs_out[k - 1] = shares[at] if shares else share(tp_peer(k))
        remote(
            rs_out.at[k - 1], rs_in.at[k - 1], rs_s.at[k - 1], rs_r.at[k - 1], "tp", tp_peer(k)
        )
    total = share(tp).astype(f32)
    for k in reversed(peers):
        drain(rs_in.at[k - 1], rs_r.at[k - 1])
        total += rs_in[k - 1].astype(f32)
    resid = (v["tokens"][:, columns(tp)].astype(f32) + total).astype(bf16)

    picked = jnp.dot(select, resid, preferred_element_type=f32)
    disp[...] = picked.reshape(n_ep, blocks, 8, width).astype(bf16)

    def dispatch(i):
        to = ep_peer(i)
        remote(disp.at[to], rows.at[tp, i], disp_s, disp_r.at[i], "ep", to)

    dispatch(partner)
    each(0, own_place, dispatch)

    def pass_on(i, here):
        for k in peers:
            remote(here, rows.at[tp, i], fwd_s.at[k - 1], fwd_r.at[i, k - 1], "tp", tp_peer(k))

    pass_on(own_place, disp.at[ep])
    rows[tp, own_place] = disp[ep]

    def forward(i):
        here = rows.at[tp, i]
        drain(here, disp_r.at[i])
        pass_on(i, here)

    forward(partner)
    each(0, own_place, forward)

    for part, members in enumerate(PASSES):
        start, count = parts[members[0]][0], sum(parts[member][1] for member in members)
        span = pl.ds(start, count)
        held = xn.at[pl.ds(0, count * slot_rows)]

        def row_values(owner):
            return rows[owner, span].astype(f32).reshape(count * slot_rows, width)

        def landed(i):
            for k in reversed(peers):
                drain(rows.at[tp_peer(k), i], fwd_r.at[i, k - 1])

        each(start, start + count, landed)
        squares = sum(row_values(owner) * row_values(owner) for owner in range(n_tp))
        squares = jnp.sum(squares, axis=1, keepdims=True)
        scale = lax.rsqrt(squares / (n_tp * width) + norm_eps)
        for owner in range(n_tp):
            cols = pl.ds(owner * width, width)
            held[:, cols] = (row_values(owner) * scale * gain_ref[:, cols]).astype(bf16)

        if part == 0:
            wait("gate")
            wait("up")
        products = (
            jnp.dot(held[...], v[name][...], preferred_element_type=f32) for name in ("gate", "up")
        )
        hidden = gated_unit(*products)
        if part == 0:
            wait("down")

        def down(owner):
            value = jnp.dot(hidden, v["down"][:, columns(owner)], preferred_element_type=f32)
            return value.reshape(count, blocks, 8, width).astype(bf16)

        def give_back(member, k):
            where = pl.ds(*parts[member])
            remote(
                back_out.at[k - 1, where],
                back_in.at[k - 1, where],
                back_s.at[member, k - 1],
                back_r.at[member, k - 1],
                "tp",
                tp_peer(k),
            )

        def hand(k, value):
            back_out[k - 1, span] = value
            give_back(members[0], k)

        ready = None
        for k in peers:
            value = down(tp_peer(k))
            if ready is not None:
                hand(*ready)
            ready = k, value
        own = down(tp)
        hand(*ready)
        for member in members[1:]:
            for k in peers:
                give_back(member, k)
        back_own[span] = own

    for part, (start, count) in enumerate(parts):
        for k in peers:
            drain(back_in.at[k - 1, pl.ds(start, count)], back_r.at[part, k - 1])

        def settle(i):
            result = back_own[i].astype(f32)
            for k in reversed(peers):
                result += back_in[k - 1, i].astype(f32)
            result = result.astype(bf16)
            if isinstance(i, int) and i == own_place:
                ret_in[ep] = result
                return
            to = ep_peer(i)
            ret_out[to] = result
            remote(ret_out.at[to], ret_in.at[ep], ret_s, ret_r.at[i], "ep", to)

        each(start, min(start + count, own_place), settle)
        if start + count == n_ep:
            settle(partner)
            settle(own_place)

    def arrived(i):
        drain(ret_in.at[ep_peer(i)], ret_r.at[i])

    each(0, own_place, arrived)
    arrived(partner)

    returned = ret_in[...].astype(f32).reshape(slots, width).astype(bf16)
    high = combine.astype(bf16)
    low = (combine - high.astype(f32)).astype(bf16)
    both = jnp.concatenate([high, low], axis=0)
    both = jnp.dot(both, returned, preferred_element_type=f32)
    out_ref[...] = (resid.astype(f32) + (both[:seqs] + both[seqs:])).astype(bf16)

    for k in peers:
        drain(mixed_ref, ag_s.at[k - 1])
        drain(rs_out.at[k - 1], rs_s.at[k - 1])
        drain(rows.at[0], fwd_s.at[k - 1])
        for part, where in enumerate(parts):
            drain(back_out.at[k - 1, pl.ds(*where)], back_s.at[part, k - 1])
    drain(disp.at[pl.ds(0, n_ep - 1)], disp_s)
    drain(ret_out.at[pl.ds(0, n_ep - 1)], ret_s)


def store(mixed_ref, re_ref, im_ref, mixed_hbm, re_hbm, im_hbm, sem):
    out = pltpu.make_async_copy(mixed_ref, mixed_hbm, sem.at[0])
    out.start()

    @pl.loop(0, re_ref.shape[0])
    def _(g):
        for i, (near, far) in enumerate(((re_ref, re_hbm), (im_ref, im_hbm))):
            pltpu.make_async_copy(near.at[g], far.at[:, g, :], sem.at[i + 1]).start()

    out.wait()
    drain(re_ref, sem.at[1])
    drain(im_ref, sem.at[2])


def local(
    tokens,
    mix_gain,
    w_in,
    decay_re,
    freq,
    log_step,
    in_re,
    in_im,
    out_re,
    out_im,
    skip,
    state_re,
    state_im,
    glu_weight,
    glu_bias,
    out_weight,
    ffn_gain,
    route,
    route_weight,
    expert_gate,
    expert_up,
    expert_down,
):
    seq_count, model_width = tokens.shape
    n_tp = lax.axis_size("tp")
    experts = lax.axis_size("ep")
    local_width = model_width // n_tp
    top_count = route.shape[1]
    slot_cap = (3 * seq_count * top_count + 2 * experts - 1) // (2 * experts)
    slot_rows = (slot_cap + 7) // 8 * 8
    chan = w_in.shape[1]
    state_block = (decay_re.shape[0], seq_count, state_re.shape[2])
    block = (slot_rows // 8, 8, local_width)
    most = max(sum(groups_of(experts)[part][1] for part in members) for members in PASSES)
    bf16 = jnp.bfloat16
    dma = pltpu.SemaphoreType.DMA
    vmem = pl.BlockSpec(memory_space=pltpu.VMEM)
    anyplace = pl.BlockSpec(memory_space=pl.ANY)
    arrays = {
        "tokens": tokens,
        "mix_gain": mix_gain[None, :],
        "w_in": w_in,
        "decay": decay_re,
        "freq": freq,
        "log_step": log_step[None, :],
        "in_re": in_re,
        "in_im": in_im,
        "out_re": out_re,
        "out_im": out_im,
        "skip": skip,
        "glu": glu_weight,
        "bias": glu_bias[None, :],
        "out_w": out_weight,
        "gain": ffn_gain[None, :],
        "route": route.T,
        "weight": route_weight.T,
        "gate": expert_gate,
        "up": expert_up,
        "down": expert_down,
    }
    arrays = [arrays[name] for name in SMALL + LATER]
    holds = [
        pltpu.VMEM(a.shape[1:] if name in ("gate", "up", "down") else a.shape, a.dtype)
        for name, a in zip(SMALL + LATER, arrays)
    ]
    mixed, new_re, new_im = pl.pallas_call(
        functools.partial(layer, n_tp, experts),
        out_shape=(
            pltpu.VMEM((seq_count, local_width), bf16),
            pltpu.VMEM(state_block, jnp.float32),
            pltpu.VMEM(state_block, jnp.float32),
        ),
        in_specs=[anyplace] * (len(arrays) + 2),
        out_specs=(vmem, vmem, vmem),
        scratch_shapes=holds
        + [
            pltpu.VMEM((seq_count, chan), bf16),
            pltpu.VMEM((n_tp - 1, seq_count, chan), bf16),
            pltpu.VMEM((n_tp - 1, seq_count, local_width), bf16),
            pltpu.VMEM((n_tp - 1, seq_count, local_width), bf16),
            pltpu.VMEM((experts,) + block, bf16),
            pltpu.VMEM((n_tp, experts) + block, bf16),
            pltpu.VMEM((most * slot_rows, model_width), bf16),
            pltpu.VMEM((n_tp - 1, experts) + block, bf16),
            pltpu.VMEM((experts,) + block, bf16),
            pltpu.VMEM((n_tp - 1, experts) + block, bf16),
            pltpu.VMEM((experts,) + block, bf16),
            pltpu.VMEM((experts,) + block, bf16),
            dma((len(arrays),)),
            dma((2,)),
            dma((n_tp - 1,)),
            dma((n_tp - 1,)),
            dma((n_tp - 1,)),
            dma((n_tp - 1,)),
            dma,
            dma((experts,)),
            dma((n_tp - 1,)),
            dma((experts, n_tp - 1)),
            dma((4, n_tp - 1)),
            dma((4, n_tp - 1)),
            dma,
            dma((experts,)),
        ],
        compiler_params=pltpu.CompilerParams(
            collective_id=0, has_side_effects=True, vmem_limit_bytes=58 * 1024 * 1024
        ),
    )(*arrays, state_re, state_im)
    results = [pltpu.with_memory_space_constraint(a, pltpu.VMEM) for a in (mixed, new_re, new_im)]
    return pl.pallas_call(
        store,
        out_shape=(
            jax.ShapeDtypeStruct((seq_count, local_width), bf16),
            jax.ShapeDtypeStruct(state_re.shape, jnp.float32),
            jax.ShapeDtypeStruct(state_im.shape, jnp.float32),
        ),
        in_specs=[vmem] * 3,
        out_specs=(anyplace,) * 3,
        scratch_shapes=[dma((3,))],
    )(*results)


def solution(mesh):
    in_specs = (
        P("ep", None),
        P(),
        P(None, "tp"),
        P("tp", None),
        P("tp", None),
        P("tp"),
        P("tp", None, None),
        P("tp", None, None),
        P("tp", None, None),
        P("tp", None, None),
        P("tp", None),
        P("ep", "tp", None),
        P("ep", "tp", None),
        P(None, "tp"),
        P("tp"),
        P("tp", None),
        P(),
        P("ep", None),
        P("ep", None),
        P("ep", None, "tp"),
        P("ep", None, "tp"),
        P("ep", "tp", None),
    )
    out_specs = (P("ep", "tp"), P("ep", "tp", None), P("ep", "tp", None))
    return jax.shard_map(local, mesh=mesh, in_specs=in_specs, out_specs=out_specs, check_vma=False)
```
